32 devices in a mesh: row: 8 (over z, core), col: 4 (over y, x).
Axes of the slice: x: 2, y: 2, z: 4, core: 2. Of those that a mesh axis runs over, the one named last changes fastest.
Arguments:
- tokens: bfloat16 [4096, 4096], P('row', 'col'), may hold values from -6 to 6
- norm_gain: float32 [4096], replicated, may hold values from 0.1 to 1.9
- out_weight: bfloat16 [4096, 4096], P(None, 'col'), may hold values from -0.09375 to 0.09375
Outputs:
- mixed: bfloat16 [4096, 4096], P('row', 'col')
The draws below stay inside these ranges and needn't reach their ends.
All inputs are finite; a program needn't handle non-finite values.
Results may differ from the reference program's by a relative error of at most 0.015.
Values may be sent and summed in bfloat16 or wider, within the bound.
A program may use at most 64 MiB of HBM per device.

```python
import jax
import jax.numpy as jnp
from jax import lax

D = 4096
GROUPS = 4
CG = 1024
SEQ = 4096


def block_levels(key, shape, shards, low, high):
    def one(position, shards_of):
        heights = jax.random.uniform(jax.random.fold_in(jax.random.fold_in(key, 6), position), (shards_of,), jnp.float32, low / len(shards), high / len(shards))
        return jnp.repeat(jnp.exp(heights), shape[position] // shards_of).reshape((-1,) + (1,) * (len(shape) - position - 1))

    level = one(*shards[0])
    for cut in shards[1:]:
        level = level * one(*cut)
    return level


def scatter_about(own_key, dims, width, reach, cuts=(), held_as=jnp.bfloat16):
    result = jax.random.normal(own_key, dims, jnp.float32) * width
    if len(cuts) > 0:
        result = block_levels(own_key, dims, cuts, -0.22, 0.18) * result
    return jnp.clip(result, min=-reach, max=reach).astype(held_as)


def setup_inputs(seed: int = 0) -> dict:
    key_of = jax.random.split(jax.random.key(seed), 4)
    return {
        "tokens": scatter_about(key_of[0], (SEQ, D), 1.0, 6.0, ((0, 8), (1, 4))),
        "norm_gain": jnp.clip(1.0 + 0.18 * jax.random.normal(key_of[1], (D,), jnp.float32), 0.1, 1.9),
        "out_weight": scatter_about(key_of[2], (D, D), D ** -0.5, 0.09375, ((1, 4),)),
    }


def reference(tokens, norm_gain, out_weight):
    values = tokens.astype(jnp.float32)
    inv_rms = lax.rsqrt(lax.optimization_barrier(jnp.mean(values * values, axis=-1, keepdims=True)) + 1e-06)
    normed = lax.optimization_barrier((values * inv_rms * norm_gain).astype(jnp.bfloat16))
    grouped = normed.astype(jnp.float32).reshape(SEQ, GROUPS, CG)
    spectrum = jnp.fft.fftn(grouped, axes=(0, 2), norm='ortho').real
    mixed_in = spectrum.reshape(SEQ, D).astype(jnp.bfloat16)
    return jnp.dot(mixed_in, out_weight, preferred_element_type=jnp.float32).astype(jnp.bfloat16)
```

```python
import math

import numpy as np

import jax
import jax.numpy as jnp
from jax import lax
from jax.sharding import PartitionSpec as P

GROUPS = 4


EPSILON = 1e-06
PRECISE = lax.Precision.HIGHEST


def phases(left_idx, right_idx, period):
    product = left_idx[:, None] * right_idx[None, :] % period
    angles = product.astype(jnp.float32) * (2.0 * math.pi / period)
    return (jnp.cos(angles), jnp.sin(angles))


def split_table(table):
    table_high = table.astype(jnp.bfloat16)
    remainder = table - table_high.astype(jnp.float32)
    table_middle = remainder.astype(jnp.bfloat16)
    table_low = (remainder - table_middle.astype(jnp.float32)).astype(jnp.bfloat16)
    return (table_high, table_middle, table_low)


def host_tables(group_len, row_count, block_len):
    seq_len = block_len * row_count
    half = group_len // 2 // row_count
    slot = np.arange(group_len)
    freq = (slot // (2 * half)) * half + slot % half
    odd = slot // half % 2 == 1
    nyquist = odd & (freq == 0)
    sine = odd & ~nyquist
    freq = np.where(nyquist, group_len // 2, freq)
    chan = np.arange(group_len)
    angle = 2 * np.pi * (chan[:, None] * freq[None, :] % group_len) / group_len
    chan_table = np.where(sine[None, :], np.sin(angle), np.cos(angle)) / np.sqrt(group_len)
    low = np.arange(block_len)
    angle = 2 * np.pi * (low[:, None] * low[None, :] % block_len) / block_len
    low_table = np.concatenate([np.cos(angle), np.sin(angle)], 1) / np.sqrt(seq_len)
    high = np.arange(row_count)
    angle = 2 * np.pi * (high[:, None] * low[None, :] % seq_len) / seq_len
    return chan_table, low_table, np.cos(angle), np.sin(angle)


def slot_facts(slot, group_len, row_count):
    half = group_len // 2 // row_count
    freq = (slot // (2 * half)) * half + slot % half
    odd = slot // half % 2 == 1
    nyquist = odd & (freq == 0)
    return jnp.where(nyquist, group_len // 2, freq), odd & ~nyquist


def folding(group_len, row_count):
    freq, sine = slot_facts(jnp.arange(group_len, dtype=jnp.int32), group_len, row_count)
    chan = jnp.arange(group_len, dtype=jnp.int32)[None, :]
    direct = chan == freq[:, None]
    mirror = chan == ((group_len - freq) % group_len)[:, None]
    signed = jnp.where(sine[:, None], -1.0, 1.0)
    return jnp.where(direct, signed, jnp.where(mirror, 1.0, 0.0)).astype(jnp.bfloat16)


def on_device_folded(tokens, norm_gain, out_weight):
    row_count = lax.axis_size("row")
    col_count = lax.axis_size("col")
    block_len, group_len = tokens.shape
    full_width = group_len * col_count
    slab = group_len // row_count
    out_width = out_weight.shape[1]
    chan_table, low_table, twist_cos, twist_sin = host_tables(group_len, row_count, block_len)
    chan_table = jnp.asarray(chan_table, jnp.bfloat16)
    low_table = jnp.asarray(low_table, jnp.bfloat16)
    twist_cos = jnp.asarray(twist_cos, jnp.float32)[:, :, None]
    twist_sin = jnp.asarray(twist_sin, jnp.float32)[:, :, None]
    values = tokens.astype(jnp.float32)
    total = lax.psum(jnp.sum(values * values, axis=-1), "col")
    inv_rms = lax.rsqrt(total / full_width + EPSILON)[:, None]
    gain = lax.dynamic_slice_in_dim(norm_gain, lax.axis_index("col") * group_len, group_len)
    normed = (values * inv_rms * gain).astype(jnp.bfloat16)
    chans = jnp.dot(normed, chan_table, preferred_element_type=jnp.float32).astype(jnp.bfloat16)
    moved = lax.all_to_all(chans, "row", split_axis=1, concat_axis=0, tiled=True)
    blocks = moved.reshape(row_count, block_len, slab).astype(jnp.float32)
    _, sine = slot_facts(
        lax.axis_index("row") * slab + jnp.arange(slab, dtype=jnp.int32), group_len, row_count
    )
    tops, bottoms = [], []
    for q in range(row_count):
        real, imag = 0.0, 0.0
        for a in range(row_count):
            angle = 2 * math.pi * (a * q % row_count) / row_count
            real = real + blocks[a] * round(math.cos(angle), 12)
            imag = imag - blocks[a] * round(math.sin(angle), 12)
        turned_real = real * twist_cos[q] + imag * twist_sin[q]
        turned_imag = imag * twist_cos[q] - real * twist_sin[q]
        tops.append(jnp.where(sine, -turned_imag, turned_real).astype(jnp.bfloat16))
        bottoms.append(jnp.where(sine, turned_real, turned_imag).astype(jnp.bfloat16))
    stacked = jnp.concatenate([jnp.concatenate(tops, 1), jnp.concatenate(bottoms, 1)], 0)
    lows = jnp.dot(low_table, stacked, preferred_element_type=jnp.float32).astype(jnp.bfloat16)
    back = lax.all_to_all(
        lows.reshape(row_count, block_len // row_count, row_count * slab),
        "row", split_axis=0, concat_axis=0, tiled=True,
    )
    gathered = lax.all_gather(back, "col", axis=0, tiled=False)
    fold = folding(group_len, row_count)
    folded = jnp.einsum(
        "sm,gme->gse", fold, out_weight.reshape(col_count, group_len, out_width),
        preferred_element_type=jnp.float32,
    ).astype(jnp.bfloat16)
    mapped = jnp.einsum(
        "gspql,gsle->pqe",
        gathered.reshape(col_count, row_count, block_len // row_count, row_count, slab),
        folded.reshape(col_count, row_count, slab, out_width),
        preferred_element_type=jnp.float32,
    )
    return mapped.astype(jnp.bfloat16).reshape(block_len, out_width)


def on_device(tokens, norm_gain, out_weight):
    row_count = lax.axis_size("row")
    col_count = lax.axis_size("col")
    block_len, local_width = tokens.shape
    full_width = local_width * col_count
    group_len = full_width // GROUPS
    share_len = block_len // col_count
    seq_len = block_len * row_count
    slab_len = full_width // row_count
    col_index = lax.axis_index("col")
    chan_idx = jnp.arange(group_len, dtype=jnp.int32)
    cosines, sines = phases(chan_idx, chan_idx, group_len)
    chan_table = jnp.concatenate([cosines, sines], axis=1) / math.sqrt(group_len)
    table_parts = split_table(chan_table)
    arranged = tokens.reshape(col_count, share_len, local_width)
    portion = lax.all_to_all(arranged, "col", split_axis=0, concat_axis=2, tiled=True)
    item_count = portion.shape[1]
    values = portion.astype(jnp.float32)
    inv_rms = lax.rsqrt(jnp.mean(values * values, axis=-1, keepdims=True) + EPSILON)
    normed = lax.optimization_barrier((values * inv_rms * norm_gain).astype(jnp.bfloat16))
    grouped = normed.reshape(item_count, GROUPS, group_len)
    result = jnp.einsum("pgm,mj->pgj", grouped, table_parts[0], preferred_element_type=jnp.float32)
    result = result + jnp.einsum(
        "pgm,mj->pgj", grouped, table_parts[1], preferred_element_type=jnp.float32
    )
    result = result + jnp.einsum(
        "pgm,mj->pgj", grouped, table_parts[2], preferred_element_type=jnp.float32
    )
    high_idx = jnp.arange(row_count, dtype=jnp.int32)
    high_cos, high_sin = phases(high_idx, high_idx, row_count)
    high_table = jnp.concatenate(
        [jnp.concatenate([high_cos, -high_sin], 1), jnp.concatenate([-high_sin, -high_cos], 1)], 0
    )
    parts = (
        lax.all_to_all(
            result[..., :group_len].reshape(1, item_count, full_width),
            "row",
            split_axis=2,
            concat_axis=0,
            tiled=True,
        ),
        lax.all_to_all(
            result[..., group_len:].reshape(1, item_count, full_width),
            "row",
            split_axis=2,
            concat_axis=0,
            tiled=True,
        ),
    )
    item_count = parts[0].shape[1]
    stacked = jnp.concatenate(parts, 0).reshape(2 * row_count, item_count * slab_len)
    result = jnp.dot(high_table, stacked, precision=PRECISE)
    real_part = result[:row_count].reshape(row_count, item_count, slab_len)
    imag_part = result[row_count:].reshape(row_count, item_count, slab_len)
    local_pos = col_index * share_len + jnp.arange(share_len, dtype=jnp.int32)
    twist_cos, twist_sin = phases(high_idx, local_pos, seq_len)
    twist_cos = twist_cos[:, :, None]
    twist_sin = twist_sin[:, :, None]
    turned_real = real_part * twist_cos + imag_part * twist_sin
    turned_imag = imag_part * twist_cos - real_part * twist_sin
    low_idx = jnp.arange(block_len, dtype=jnp.int32)
    low_cos, low_sin = phases(low_idx, low_idx, block_len)
    low_cos = low_cos / math.sqrt(seq_len)
    low_sin = low_sin / math.sqrt(seq_len)
    low_table = jnp.concatenate([low_cos, low_sin], 1)
    stacked = jnp.concatenate(
        (
            lax.all_to_all(turned_real, "col", split_axis=0, concat_axis=1, tiled=True),
            lax.all_to_all(turned_imag, "col", split_axis=0, concat_axis=1, tiled=True),
        ),
        1,
    )
    finished = (jnp.einsum("ks,asc->akc", low_table, stacked, precision=PRECISE),)[0]
    spectrum = finished.astype(jnp.bfloat16)
    returned = lax.all_to_all(spectrum, "row", split_axis=1, concat_axis=2, tiled=True)
    mapped = jnp.einsum(
        "akd,de->kae",
        lax.all_gather(returned, "col", axis=0, tiled=True),
        out_weight,
        preferred_element_type=jnp.float32,
    )
    return mapped.astype(jnp.bfloat16).reshape(block_len, local_width)


def solution(mesh):
    def body(tokens, norm_gain, out_weight):
        whole_groups = tokens.shape[1] * GROUPS == out_weight.shape[0]
        program = on_device_folded if whole_groups else on_device
        return program(tokens, norm_gain, out_weight)

    placed = (P("row", "col"), P(), P(None, "col"))
    return jax.shard_map(
        body, mesh=mesh, in_specs=placed, out_specs=P("row", "col"), check_vma=False
    )
```

```python
import functools
import math

import numpy as np

import jax
import jax.numpy as jnp
from jax import lax
from jax.experimental import pallas as pl
from jax.experimental.pallas import tpu as pltpu
from jax.sharding import PartitionSpec as P

GROUPS = 4


EPSILON = 1e-06
PRECISE = lax.Precision.HIGHEST


def phases(left_idx, right_idx, period):
    product = left_idx[:, None] * right_idx[None, :] % period
    angles = product.astype(jnp.float32) * (2.0 * math.pi / period)
    return (jnp.cos(angles), jnp.sin(angles))


def split_table(table):
    table_high = table.astype(jnp.bfloat16)
    remainder = table - table_high.astype(jnp.float32)
    table_middle = remainder.astype(jnp.bfloat16)
    table_low = (remainder - table_middle.astype(jnp.float32)).astype(jnp.bfloat16)
    return (table_high, table_middle, table_low)


def host_tables(group_len, row_count, block_len):
    seq_len = block_len * row_count
    half = group_len // 2 // row_count
    slot = np.arange(group_len)
    freq = (slot // (2 * half)) * half + slot % half
    odd = slot // half % 2 == 1
    nyquist = odd & (freq == 0)
    sine = odd & ~nyquist
    freq = np.where(nyquist, group_len // 2, freq)
    chan = np.arange(group_len)
    angle = 2 * np.pi * (chan[:, None] * freq[None, :] % group_len) / group_len
    chan_table = np.where(sine[None, :], np.sin(angle), np.cos(angle)) / np.sqrt(group_len)
    low = np.arange(block_len)
    angle = 2 * np.pi * (low[:, None] * low[None, :] % block_len) / block_len
    low_table = np.concatenate([np.cos(angle), np.sin(angle)], 1) / np.sqrt(seq_len)
    high = np.arange(row_count)
    angle = 2 * np.pi * (high[:, None] * low[None, :] % seq_len) / seq_len
    return chan_table, low_table, np.cos(angle), np.sin(angle)


def slot_facts(slot, group_len, row_count):
    half = group_len // 2 // row_count
    freq = (slot // (2 * half)) * half + slot % half
    odd = slot // half % 2 == 1
    nyquist = odd & (freq == 0)
    return jnp.where(nyquist, group_len // 2, freq), odd & ~nyquist


def folding(group_len, row_count):
    freq, sine = slot_facts(jnp.arange(group_len, dtype=jnp.int32), group_len, row_count)
    chan = jnp.arange(group_len, dtype=jnp.int32)[None, :]
    direct = chan == freq[:, None]
    mirror = chan == ((group_len - freq) % group_len)[:, None]
    signed = jnp.where(sine[:, None], -1.0, 1.0)
    return jnp.where(direct, signed, jnp.where(mirror, 1.0, 0.0)).astype(jnp.bfloat16)


def on_device_folded(tokens, norm_gain, out_weight):
    row_count = lax.axis_size("row")
    col_count = lax.axis_size("col")
    block_len, group_len = tokens.shape
    full_width = group_len * col_count
    slab = group_len // row_count
    out_width = out_weight.shape[1]
    chan_table, low_table, twist_cos, twist_sin = host_tables(group_len, row_count, block_len)
    chan_table = jnp.asarray(chan_table, jnp.bfloat16)
    low_table = jnp.asarray(low_table, jnp.bfloat16)
    twist_cos = jnp.asarray(twist_cos, jnp.float32)[:, :, None]
    twist_sin = jnp.asarray(twist_sin, jnp.float32)[:, :, None]
    values = tokens.astype(jnp.float32)
    total = lax.psum(jnp.sum(values * values, axis=-1), "col")
    inv_rms = lax.rsqrt(total / full_width + EPSILON)[:, None]
    gain = lax.dynamic_slice_in_dim(norm_gain, lax.axis_index("col") * group_len, group_len)
    normed = (values * inv_rms * gain).astype(jnp.bfloat16)
    chans = jnp.dot(normed, chan_table, preferred_element_type=jnp.float32).astype(jnp.bfloat16)
    moved = lax.all_to_all(chans, "row", split_axis=1, concat_axis=0, tiled=True)
    blocks = moved.reshape(row_count, block_len, slab).astype(jnp.float32)
    _, sine = slot_facts(
        lax.axis_index("row") * slab + jnp.arange(slab, dtype=jnp.int32), group_len, row_count
    )
    tops, bottoms = [], []
    for q in range(row_count):
        real, imag = 0.0, 0.0
        for a in range(row_count):
            angle = 2 * math.pi * (a * q % row_count) / row_count
            real = real + blocks[a] * round(math.cos(angle), 12)
            imag = imag - blocks[a] * round(math.sin(angle), 12)
        turned_real = real * twist_cos[q] + imag * twist_sin[q]
        turned_imag = imag * twist_cos[q] - real * twist_sin[q]
        tops.append(jnp.where(sine, -turned_imag, turned_real).astype(jnp.bfloat16))
        bottoms.append(jnp.where(sine, turned_real, turned_imag).astype(jnp.bfloat16))
    stacked = jnp.concatenate([jnp.concatenate(tops, 1), jnp.concatenate(bottoms, 1)], 0)
    lows = jnp.dot(low_table, stacked, preferred_element_type=jnp.float32).astype(jnp.bfloat16)
    back = lax.all_to_all(
        lows.reshape(row_count, block_len // row_count, row_count * slab),
        "row", split_axis=0, concat_axis=0, tiled=True,
    )
    gathered = lax.all_gather(back, "col", axis=0, tiled=False)
    fold = folding(group_len, row_count)
    folded = jnp.einsum(
        "sm,gme->gse", fold, out_weight.reshape(col_count, group_len, out_width),
        preferred_element_type=jnp.float32,
    ).astype(jnp.bfloat16)
    mapped = jnp.einsum(
        "gspql,gsle->pqe",
        gathered.reshape(col_count, row_count, block_len // row_count, row_count, slab),
        folded.reshape(col_count, row_count, slab, out_width),
        preferred_element_type=jnp.float32,
    )
    return mapped.astype(jnp.bfloat16).reshape(block_len, out_width)


MESH = pl.DeviceIdType.MESH
F32 = jnp.float32
BF16 = jnp.bfloat16


def fused_kernel(
    dims, x_ref, gain_ref, table_ref, low_ref, twist_ref, w_hbm, out_ref,
    w_ref, fold_ref, folded, send1, recv1, sums, stacked, send2, lhs, acc, spread,
    w_sem, s_send, s_recv, a_send, a_recv, b_send, b_recv, g_send, g_recv, l_sem,
):
    row_count, col_count = dims
    block_len, group_len = x_ref.shape
    full_width = group_len * col_count
    slab = group_len // row_count
    half = slab // 2
    pair = 2 * slab
    chips = row_count // 2
    part = block_len // row_count
    out_width = out_ref.shape[1]
    r = lax.axis_index("row")
    c = lax.axis_index("col")
    z = r // 2
    other = 2 * z + 1 - r % 2
    x_next = 2 * (c // 2) + 1 - c % 2
    y_next = 2 * (1 - c // 2) + c % 2
    diagonal = 2 * (1 - c // 2) + 1 - c % 2
    col_peers = (x_next, y_next, diagonal)
    w_copy = pltpu.make_async_copy(w_hbm, w_ref, w_sem)
    w_copy.start()

    barrier = pltpu.get_barrier_semaphore()
    for step in range(1, row_count):
        pl.semaphore_signal(
            barrier, inc=1, device_id=(lax.rem(r + step, row_count), c), device_id_type=MESH
        )
    for peer in col_peers:
        pl.semaphore_signal(barrier, inc=1, device_id=(r, peer), device_id_type=MESH)
    pl.semaphore_wait(barrier, row_count + col_count - 2)

    values = x_ref[...].astype(F32)
    squares = values * values
    top = squares.astype(BF16)
    rest = (squares - top.astype(F32)).astype(BF16)
    ones = jnp.ones((16, group_len), BF16)
    lanes = (((1,), (1,)), ((), ()))
    own = lax.dot_general(ones, top, lanes, preferred_element_type=F32)
    own = own + lax.dot_general(ones, rest, lanes, preferred_element_type=F32)
    sums[c] = own[:8]
    sum_copies = []
    for k, peer in enumerate(col_peers):
        copy = pltpu.make_async_remote_copy(
            src_ref=sums.at[c], dst_ref=sums.at[c], send_sem=s_send.at[k], recv_sem=s_recv.at[k],
            device_id=(r, peer), device_id_type=MESH,
        )
        copy.start()
        sum_copies.append(copy)

    gain = gain_ref[:, pl.ds(pl.multiple_of(c * group_len, group_len), group_len)]
    scaled = (values * gain).astype(BF16)
    far_first = sorted(range(chips), key=lambda d: -min(d, chips - d))
    first_copies = []
    inv = None
    for d in far_first:
        chip = lax.rem(z + d, chips)
        product = jnp.dot(
            scaled, table_ref[:, pl.ds(pl.multiple_of(chip * pair, pair), pair)],
            preferred_element_type=F32,
        )
        if inv is None:
            for copy in sum_copies:
                copy.wait_recv()
            total = sums[0, :1, :]
            for k in range(1, col_count):
                total = total + sums[k, :1, :]
            inv = lax.rsqrt(total / full_width + EPSILON)
            inv = jnp.transpose(jnp.broadcast_to(inv, (128, block_len)))
        send1[2 * chip] = (product[:, :slab] * inv).astype(BF16)
        send1[2 * chip + 1] = (product[:, slab:] * inv).astype(BF16)
        for target, slot in ([(2 * chip, 2 * d), (2 * chip + 1, 2 * d + 1)] if d else [(other, 0)]):
            copy = pltpu.make_async_remote_copy(
                src_ref=send1.at[target], dst_ref=recv1.at[r], send_sem=a_send.at[slot],
                recv_sem=a_recv.at[slot] if d == 0 else a_recv.at[2 * d + r % 2],
                device_id=(target, c), device_id_type=MESH,
            )
            copy.start()
            first_copies.append(copy)
    stay1 = pltpu.make_async_copy(send1.at[r], recv1.at[r], l_sem.at[0])
    stay1.start()

    for t in range(chips):
        slot = t * pair + lax.broadcasted_iota(jnp.int32, (pair, 4 * slab), 0)
        column = lax.broadcasted_iota(jnp.int32, (pair, 4 * slab), 1)
        within = slot % slab
        freq = (slot // slab) * half + within % half
        odd = within >= half
        nyquist = odd & (freq == 0)
        high = min(group_len - slab * (t + 1), group_len - pair)
        direct = (column == freq - slab * t) & ~nyquist & (column < slab)
        mirror = (column - slab + high == group_len - freq) & (freq > 0)
        mirror = mirror & (column >= slab) & (column < 3 * slab)
        middle = nyquist & (column == 3 * slab)
        signed = jnp.where(odd, -1.0, 1.0)
        fold_ref[t] = jnp.where(direct, signed, jnp.where(mirror | middle, 1.0, 0.0)).astype(BF16)

    w_copy.wait()
    wide = 256
    pieces = out_width // wide

    def fold_step(i, carry):
        base = pl.multiple_of((i // pieces) * group_len, group_len)
        cols = pl.ds(pl.multiple_of((i % pieces) * wide, wide), wide)
        for t in range(chips):
            high = min(group_len - slab * (t + 1), group_len - pair)
            taken = [w_ref[pl.ds(base + slab * t, slab), cols], w_ref[pl.ds(base + high, pair), cols]]
            if t == 0:
                taken.append(w_ref[pl.ds(base + group_len // 2, slab), cols])
            depth = slab * (4 if t == 0 else 3)
            folded[pl.ds(base + pair * t, pair), cols] = jnp.dot(
                fold_ref[t, :, :depth], jnp.concatenate(taken, 0), preferred_element_type=F32
            ).astype(BF16)
        return carry

    lax.fori_loop(0, col_count * pieces, fold_step, 0)

    def arrived(ref, semaphore):
        pltpu.make_async_remote_copy(
            src_ref=ref, dst_ref=ref, send_sem=l_sem.at[0], recv_sem=semaphore,
            device_id=(other, c), device_id_type=MESH,
        ).wait_recv()

    def block_of(d, i):
        return 2 * lax.rem(z - d + chips, chips) + i

    stay1.wait()
    arrived(recv1.at[other], a_recv.at[0])
    for d in range(1, chips):
        for i in range(2):
            arrived(recv1.at[block_of(d, i)], a_recv.at[2 * d + i])
    tile = 32
    lane = lax.broadcasted_iota(jnp.int32, (tile, slab), 1)
    sine = (lane > half) | ((lane == half) & (r > 0))

    def turn_step(i, carry):
        rows = pl.ds(pl.multiple_of(i * tile, tile), tile)
        below = pl.ds(pl.multiple_of(block_len + i * tile, tile), tile)
        blocks = [recv1[a, rows, :].astype(F32) for a in range(row_count)]
        middle = row_count // 2
        even = [blocks[a] + blocks[row_count - a] for a in range(1, middle)]
        odd = [blocks[a] - blocks[row_count - a] for a in range(1, middle)]
        ends = (blocks[0] + blocks[middle], blocks[0] - blocks[middle])
        twist = twist_ref[rows, :]
        for q in range(middle + 1):
            real = ends[q % 2]
            imag = None
            for a in range(1, middle):
                angle = 2 * math.pi * (a * q % row_count) / row_count
                cosine, sinus = round(math.cos(angle), 12), round(math.sin(angle), 12)
                if cosine:
                    real = real + even[a - 1] * cosine
                if sinus:
                    term = odd[a - 1] * -sinus
                    imag = term if imag is None else imag + term
            for k, sign in ((q, 1.0), (row_count - q, -1.0)):
                if k == row_count or (sign < 0 and k == q):
                    continue
                cosine, sinus = twist[:, k : k + 1], twist[:, row_count + k : row_count + k + 1]
                if imag is None:
                    turned_real, turned_imag = real * cosine, -(real * sinus)
                else:
                    turned_real = real * cosine + imag * (sinus * sign)
                    turned_imag = imag * (cosine * sign) - real * sinus
                cols = pl.ds(k * slab, slab)
                stacked[rows, cols] = jnp.where(sine, -turned_imag, turned_real).astype(BF16)
                stacked[below, cols] = jnp.where(sine, turned_real, turned_imag).astype(BF16)
        return carry

    lax.fori_loop(0, block_len // tile, turn_step, 0)

    def lanes_of(index):
        return pl.ds(pl.multiple_of(index * slab, slab), slab)

    second_copies = {}
    for d in far_first:
        chip = lax.rem(z + d, chips)
        lows = jnp.dot(
            low_ref[pl.ds(pl.multiple_of(chip * 2 * part, 2 * part), 2 * part), :], stacked[...],
            preferred_element_type=F32,
        ).astype(BF16)
        for i in range(2):
            for q in range(row_count):
                send2[2 * chip + i, q] = lows[i * part : (i + 1) * part, q * slab : (q + 1) * slab]
        for target, slot in ([(2 * chip, 2 * d), (2 * chip + 1, 2 * d + 1)] if d else [(other, 0)]):
            copy = pltpu.make_async_remote_copy(
                src_ref=send2.at[target], dst_ref=lhs.at[c, :, :, lanes_of(r)],
                send_sem=b_send.at[slot],
                recv_sem=b_recv.at[slot] if d == 0 else b_recv.at[2 * d + r % 2],
                device_id=(target, c), device_id_type=MESH,
            )
            copy.start()
            second_copies[slot] = copy
    stay2 = pltpu.make_async_copy(send2.at[r], lhs.at[c, :, :, lanes_of(r)], l_sem.at[1])
    stay2.start()

    sends = []

    def share(origin, source, block, target, out_slot, in_slot):
        copy = pltpu.make_async_remote_copy(
            src_ref=source, dst_ref=lhs.at[origin, :, :, lanes_of(block)],
            send_sem=g_send.at[out_slot], recv_sem=g_recv.at[in_slot],
            device_id=(r, target), device_id_type=MESH,
        )
        copy.start()
        sends.append(copy)
        return copy

    def held(origin, block):
        return lhs.at[origin, :, :, lanes_of(block)]

    order = [(None, r), (None, other)]
    for d in sorted(range(1, chips), key=lambda d: min(d, chips - d)):
        order += [((2 * d + i), block_of(d, i)) for i in range(2)]
    count = len(order)
    from_x, from_y, from_far = [], [], []
    for n in range(count + 1):
        if n < count:
            slot, block = order[n]
            if n == 0:
                stay2.wait()
            else:
                arrived(held(c, block), b_recv.at[0 if n == 1 else slot])
            source = held(c, block)
            from_x.append(share(c, source, block, x_next, n, n))
            from_y.append(share(c, source, block, y_next, count + n, count + n))
        if n:
            _, block = order[n - 1]
            slot = 2 * count + n - 1
            if n % 2:
                from_x[n - 1].wait_recv()
                from_far.append(share(x_next, held(x_next, block), block, y_next, slot, slot))
            else:
                from_y[n - 1].wait_recv()
                from_far.append(share(y_next, held(y_next, block), block, x_next, slot, slot))

    def multiply(origin, first, last):
        base = pl.multiple_of(origin * group_len, group_len)

        def step(i, carry):
            cols = pl.ds(pl.multiple_of(i * wide, wide), wide)
            left = lhs[origin].reshape(block_len, group_len)
            value = jnp.dot(left, folded[pl.ds(base, group_len), cols], preferred_element_type=F32)
            if not first:
                value = acc[:, cols] + value
            if not last:
                acc[:, cols] = value
            else:
                for q in range(row_count):
                    for j in range(wide // 128):
                        spread[j, pl.ds(q, part, stride=row_count), :] = value[
                            q * part : (q + 1) * part, j * 128 : (j + 1) * 128
                        ]
                for j in range(wide // 128):
                    at = pl.ds(pl.multiple_of(i * wide + j * 128, 128), 128)
                    out_ref[:, at] = spread[j].astype(BF16)
            return carry

        lax.fori_loop(0, pieces, step, 0)

    multiply(c, True, False)
    for n in range(1, count, 2):
        from_x[n].wait_recv()
    multiply(x_next, False, False)
    for n in range(0, count, 2):
        from_y[n].wait_recv()
    multiply(y_next, False, False)
    for copy in from_far:
        copy.wait_recv()
    multiply(diagonal, False, True)

    for copy in sum_copies + first_copies + list(second_copies.values()) + sends:
        copy.wait_send()


def on_device_fused(tokens, norm_gain, out_weight):
    row_count = lax.axis_size("row")
    col_count = lax.axis_size("col")
    block_len, group_len = tokens.shape
    out_width = out_weight.shape[1]
    slab = group_len // row_count
    part = block_len // row_count
    chan_table, low_table, twist_cos, twist_sin = host_tables(group_len, row_count, block_len)
    twist = np.zeros((block_len, 128), np.float32)
    twist[:, :row_count] = twist_cos.T
    twist[:, row_count : 2 * row_count] = twist_sin.T
    vmem = pl.BlockSpec(memory_space=pltpu.VMEM)
    dma = pltpu.SemaphoreType.DMA
    return pl.pallas_call(
        functools.partial(fused_kernel, (row_count, col_count)),
        out_shape=jax.ShapeDtypeStruct((block_len, out_width), BF16),
        in_specs=[vmem] * 5 + [pl.BlockSpec(memory_space=pl.ANY)],
        out_specs=vmem,
        scratch_shapes=[
            pltpu.VMEM(out_weight.shape, BF16),
            pltpu.VMEM((row_count // 2, 2 * slab, 4 * slab), BF16),
            pltpu.VMEM(out_weight.shape, BF16),
            pltpu.VMEM((row_count, block_len, slab), BF16),
            pltpu.VMEM((row_count, block_len, slab), BF16),
            pltpu.VMEM((col_count, 8, block_len), F32),
            pltpu.VMEM((2 * block_len, row_count * slab), BF16),
            pltpu.VMEM((row_count, row_count, part, slab), BF16),
            pltpu.VMEM((col_count, row_count, part, group_len), BF16),
            pltpu.VMEM((block_len, out_width), F32),
            pltpu.VMEM((2, block_len, 128), F32),
            dma, dma((col_count - 1,)), dma((col_count - 1,)),
            dma((row_count,)), dma((row_count,)), dma((row_count,)), dma((row_count,)),
            dma((3 * row_count,)), dma((3 * row_count,)), dma((2,)),
        ],
        compiler_params=pltpu.CompilerParams(
            collective_id=0, has_side_effects=True, vmem_limit_bytes=60 * 1024 * 1024
        ),
    )(
        tokens, norm_gain[None, :], jnp.asarray(chan_table, BF16), jnp.asarray(low_table, BF16),
        jnp.asarray(twist), out_weight,
    )


def on_device(tokens, norm_gain, out_weight):
    row_count = lax.axis_size("row")
    col_count = lax.axis_size("col")
    block_len, local_width = tokens.shape
    full_width = local_width * col_count
    group_len = full_width // GROUPS
    share_len = block_len // col_count
    seq_len = block_len * row_count
    slab_len = full_width // row_count
    col_index = lax.axis_index("col")
    chan_idx = jnp.arange(group_len, dtype=jnp.int32)
    cosines, sines = phases(chan_idx, chan_idx, group_len)
    chan_table = jnp.concatenate([cosines, sines], axis=1) / math.sqrt(group_len)
    table_parts = split_table(chan_table)
    arranged = tokens.reshape(col_count, share_len, local_width)
    portion = lax.all_to_all(arranged, "col", split_axis=0, concat_axis=2, tiled=True)
    item_count = portion.shape[1]
    values = portion.astype(jnp.float32)
    inv_rms = lax.rsqrt(jnp.mean(values * values, axis=-1, keepdims=True) + EPSILON)
    normed = lax.optimization_barrier((values * inv_rms * norm_gain).astype(jnp.bfloat16))
    grouped = normed.reshape(item_count, GROUPS, group_len)
    result = jnp.einsum("pgm,mj->pgj", grouped, table_parts[0], preferred_element_type=jnp.float32)
    result = result + jnp.einsum(
        "pgm,mj->pgj", grouped, table_parts[1], preferred_element_type=jnp.float32
    )
    result = result + jnp.einsum(
        "pgm,mj->pgj", grouped, table_parts[2], preferred_element_type=jnp.float32
    )
    high_idx = jnp.arange(row_count, dtype=jnp.int32)
    high_cos, high_sin = phases(high_idx, high_idx, row_count)
    high_table = jnp.concatenate(
        [jnp.concatenate([high_cos, -high_sin], 1), jnp.concatenate([-high_sin, -high_cos], 1)], 0
    )
    parts = (
        lax.all_to_all(
            result[..., :group_len].reshape(1, item_count, full_width),
            "row",
            split_axis=2,
            concat_axis=0,
            tiled=True,
        ),
        lax.all_to_all(
            result[..., group_len:].reshape(1, item_count, full_width),
            "row",
            split_axis=2,
            concat_axis=0,
            tiled=True,
        ),
    )
    item_count = parts[0].shape[1]
    stacked = jnp.concatenate(parts, 0).reshape(2 * row_count, item_count * slab_len)
    result = jnp.dot(high_table, stacked, precision=PRECISE)
    real_part = result[:row_count].reshape(row_count, item_count, slab_len)
    imag_part = result[row_count:].reshape(row_count, item_count, slab_len)
    local_pos = col_index * share_len + jnp.arange(share_len, dtype=jnp.int32)
    twist_cos, twist_sin = phases(high_idx, local_pos, seq_len)
    twist_cos = twist_cos[:, :, None]
    twist_sin = twist_sin[:, :, None]
    turned_real = real_part * twist_cos + imag_part * twist_sin
    turned_imag = imag_part * twist_cos - real_part * twist_sin
    low_idx = jnp.arange(block_len, dtype=jnp.int32)
    low_cos, low_sin = phases(low_idx, low_idx, block_len)
    low_cos = low_cos / math.sqrt(seq_len)
    low_sin = low_sin / math.sqrt(seq_len)
    low_table = jnp.concatenate([low_cos, low_sin], 1)
    stacked = jnp.concatenate(
        (
            lax.all_to_all(turned_real, "col", split_axis=0, concat_axis=1, tiled=True),
            lax.all_to_all(turned_imag, "col", split_axis=0, concat_axis=1, tiled=True),
        ),
        1,
    )
    finished = (jnp.einsum("ks,asc->akc", low_table, stacked, precision=PRECISE),)[0]
    spectrum = finished.astype(jnp.bfloat16)
    returned = lax.all_to_all(spectrum, "row", split_axis=1, concat_axis=2, tiled=True)
    mapped = jnp.einsum(
        "akd,de->kae",
        lax.all_gather(returned, "col", axis=0, tiled=True),
        out_weight,
        preferred_element_type=jnp.float32,
    )
    return mapped.astype(jnp.bfloat16).reshape(block_len, local_width)


def solution(mesh):
    def body(tokens, norm_gain, out_weight):
        whole_groups = tokens.shape[1] * GROUPS == out_weight.shape[0]
        slab = tokens.shape[1] // mesh.shape["row"]
        program = on_device_folded if whole_groups else on_device
        if whole_groups and slab == 128 and mesh.shape["col"] == 4 and mesh.shape["row"] == 8:
            program = on_device_fused
        return program(tokens, norm_gain, out_weight)

    placed = (P("row", "col"), P(), P(None, "col"))
    return jax.shard_map(
        body, mesh=mesh, in_specs=placed, out_specs=P("row", "col"), check_vma=False
    )
```

```python
import functools
import math

import numpy as np

import jax
import jax.numpy as jnp
from jax import lax
from jax.experimental import pallas as pl
from jax.experimental.pallas import tpu as pltpu
from jax.sharding import PartitionSpec as P

GROUPS = 4


EPSILON = 1e-06
PRECISE = lax.Precision.HIGHEST


def phases(left_idx, right_idx, period):
    product = left_idx[:, None] * right_idx[None, :] % period
    angles = product.astype(jnp.float32) * (2.0 * math.pi / period)
    return (jnp.cos(angles), jnp.sin(angles))


def split_table(table):
    table_high = table.astype(jnp.bfloat16)
    remainder = table - table_high.astype(jnp.float32)
    table_middle = remainder.astype(jnp.bfloat16)
    table_low = (remainder - table_middle.astype(jnp.float32)).astype(jnp.bfloat16)
    return (table_high, table_middle, table_low)


def host_tables(group_len, row_count, block_len):
    seq_len = block_len * row_count
    half = group_len // 2 // row_count
    slot = np.arange(group_len)
    freq = (slot // (2 * half)) * half + slot % half
    odd = slot // half % 2 == 1
    nyquist = odd & (freq == 0)
    sine = odd & ~nyquist
    freq = np.where(nyquist, group_len // 2, freq)
    chan = np.arange(group_len)
    angle = 2 * np.pi * (chan[:, None] * freq[None, :] % group_len) / group_len
    chan_table = np.where(sine[None, :], np.sin(angle), np.cos(angle)) / np.sqrt(group_len)
    low = np.arange(block_len)
    angle = 2 * np.pi * (low[:, None] * low[None, :] % block_len) / block_len
    low_table = np.concatenate([np.cos(angle), np.sin(angle)], 1) / np.sqrt(seq_len)
    high = np.arange(row_count)
    angle = 2 * np.pi * (high[:, None] * low[None, :] % seq_len) / seq_len
    return chan_table, low_table, np.cos(angle), np.sin(angle)


def slot_facts(slot, group_len, row_count):
    half = group_len // 2 // row_count
    freq = (slot // (2 * half)) * half + slot % half
    odd = slot // half % 2 == 1
    nyquist = odd & (freq == 0)
    return jnp.where(nyquist, group_len // 2, freq), odd & ~nyquist


def folding(group_len, row_count):
    freq, sine = slot_facts(jnp.arange(group_len, dtype=jnp.int32), group_len, row_count)
    chan = jnp.arange(group_len, dtype=jnp.int32)[None, :]
    direct = chan == freq[:, None]
    mirror = chan == ((group_len - freq) % group_len)[:, None]
    signed = jnp.where(sine[:, None], -1.0, 1.0)
    return jnp.where(direct, signed, jnp.where(mirror, 1.0, 0.0)).astype(jnp.bfloat16)


def on_device_folded(tokens, norm_gain, out_weight):
    row_count = lax.axis_size("row")
    col_count = lax.axis_size("col")
    block_len, group_len = tokens.shape
    full_width = group_len * col_count
    slab = group_len // row_count
    out_width = out_weight.shape[1]
    chan_table, low_table, twist_cos, twist_sin = host_tables(group_len, row_count, block_len)
    chan_table = jnp.asarray(chan_table, jnp.bfloat16)
    low_table = jnp.asarray(low_table, jnp.bfloat16)
    twist_cos = jnp.asarray(twist_cos, jnp.float32)[:, :, None]
    twist_sin = jnp.asarray(twist_sin, jnp.float32)[:, :, None]
    values = tokens.astype(jnp.float32)
    total = lax.psum(jnp.sum(values * values, axis=-1), "col")
    inv_rms = lax.rsqrt(total / full_width + EPSILON)[:, None]
    gain = lax.dynamic_slice_in_dim(norm_gain, lax.axis_index("col") * group_len, group_len)
    normed = (values * inv_rms * gain).astype(jnp.bfloat16)
    chans = jnp.dot(normed, chan_table, preferred_element_type=jnp.float32).astype(jnp.bfloat16)
    moved = lax.all_to_all(chans, "row", split_axis=1, concat_axis=0, tiled=True)
    blocks = moved.reshape(row_count, block_len, slab).astype(jnp.float32)
    _, sine = slot_facts(
        lax.axis_index("row") * slab + jnp.arange(slab, dtype=jnp.int32), group_len, row_count
    )
    tops, bottoms = [], []
    for q in range(row_count):
        real, imag = 0.0, 0.0
        for a in range(row_count):
            angle = 2 * math.pi * (a * q % row_count) / row_count
            real = real + blocks[a] * round(math.cos(angle), 12)
            imag = imag - blocks[a] * round(math.sin(angle), 12)
        turned_real = real * twist_cos[q] + imag * twist_sin[q]
        turned_imag = imag * twist_cos[q] - real * twist_sin[q]
        tops.append(jnp.where(sine, -turned_imag, turned_real).astype(jnp.bfloat16))
        bottoms.append(jnp.where(sine, turned_real, turned_imag).astype(jnp.bfloat16))
    stacked = jnp.concatenate([jnp.concatenate(tops, 1), jnp.concatenate(bottoms, 1)], 0)
    lows = jnp.dot(low_table, stacked, preferred_element_type=jnp.float32).astype(jnp.bfloat16)
    back = lax.all_to_all(
        lows.reshape(row_count, block_len // row_count, row_count * slab),
        "row", split_axis=0, concat_axis=0, tiled=True,
    )
    gathered = lax.all_gather(back, "col", axis=0, tiled=False)
    fold = folding(group_len, row_count)
    folded = jnp.einsum(
        "sm,gme->gse", fold, out_weight.reshape(col_count, group_len, out_width),
        preferred_element_type=jnp.float32,
    ).astype(jnp.bfloat16)
    mapped = jnp.einsum(
        "gspql,gsle->pqe",
        gathered.reshape(col_count, row_count, block_len // row_count, row_count, slab),
        folded.reshape(col_count, row_count, slab, out_width),
        preferred_element_type=jnp.float32,
    )
    return mapped.astype(jnp.bfloat16).reshape(block_len, out_width)


MESH = pl.DeviceIdType.MESH
F32 = jnp.float32
BF16 = jnp.bfloat16


def fused_kernel(
    dims, x_ref, gain_ref, table_hbm, low_hbm, twist_hbm, w_hbm, out_ref,
    table_ref, low_ref, twist_ref, w_ref, fold_ref, folded, send1, recv1, sums, stacked, send2, lhs, acc, spread,
    w_sem, s_send, s_recv, a_send, a_recv, b_send, b_recv, g_send, g_recv, l_sem,
):
    row_count, col_count = dims
    block_len, group_len = x_ref.shape
    full_width = group_len * col_count
    slab = group_len // row_count
    half = slab // 2
    pair = 2 * slab
    chips = row_count // 2
    part = block_len // row_count
    out_width = out_ref.shape[1]
    r = lax.axis_index("row")
    c = lax.axis_index("col")
    z = r // 2
    other = 2 * z + 1 - r % 2
    x_next = 2 * (c // 2) + 1 - c % 2
    y_next = 2 * (1 - c // 2) + c % 2
    diagonal = 2 * (1 - c // 2) + 1 - c % 2
    col_peers = (x_next, y_next, diagonal)
    table_copy = pltpu.make_async_copy(table_hbm, table_ref, l_sem.at[2])
    w_copy = pltpu.make_async_copy(w_hbm, w_ref, w_sem)
    low_copy = pltpu.make_async_copy(low_hbm, low_ref, l_sem.at[3])
    twist_copy = pltpu.make_async_copy(twist_hbm, twist_ref, l_sem.at[4])
    for copy in (table_copy, w_copy, low_copy, twist_copy):
        copy.start()

    barrier = pltpu.get_barrier_semaphore()
    for step in range(1, row_count):
        pl.semaphore_signal(
            barrier, inc=1, device_id=(lax.rem(r + step, row_count), c), device_id_type=MESH
        )
    for peer in col_peers:
        pl.semaphore_signal(barrier, inc=1, device_id=(r, peer), device_id_type=MESH)
    pl.semaphore_wait(barrier, row_count + col_count - 2)

    values = x_ref[...].astype(F32)
    squares = values * values
    top = squares.astype(BF16)
    rest = (squares - top.astype(F32)).astype(BF16)
    ones = jnp.ones((16, group_len), BF16)
    lanes = (((1,), (1,)), ((), ()))
    own = lax.dot_general(ones, top, lanes, preferred_element_type=F32)
    own = own + lax.dot_general(ones, rest, lanes, preferred_element_type=F32)
    sums[c] = own[:8]
    sum_copies = []
    for k, peer in enumerate(col_peers):
        copy = pltpu.make_async_remote_copy(
            src_ref=sums.at[c], dst_ref=sums.at[c], send_sem=s_send.at[k], recv_sem=s_recv.at[k],
            device_id=(r, peer), device_id_type=MESH,
        )
        copy.start()
        sum_copies.append(copy)

    gain = gain_ref[:, pl.ds(pl.multiple_of(c * group_len, group_len), group_len)]
    scaled = (values * gain).astype(BF16)
    far_first = sorted(range(chips), key=lambda d: -min(d, chips - d))
    first_copies = []
    inv = None
    table_copy.wait()
    for d in far_first:
        chip = lax.rem(z + d, chips)
        product = jnp.dot(
            scaled, table_ref[:, pl.ds(pl.multiple_of(chip * pair, pair), pair)],
            preferred_element_type=F32,
        )
        if inv is None:
            for copy in sum_copies:
                copy.wait_recv()
            total = sums[0, :1, :]
            for k in range(1, col_count):
                total = total + sums[k, :1, :]
            inv = lax.rsqrt(total / full_width + EPSILON)
            inv = jnp.transpose(jnp.broadcast_to(inv, (128, block_len)))
        send1[2 * chip] = (product[:, :slab] * inv).astype(BF16)
        send1[2 * chip + 1] = (product[:, slab:] * inv).astype(BF16)
        for target, slot in ([(2 * chip, 2 * d), (2 * chip + 1, 2 * d + 1)] if d else [(other, 0)]):
            copy = pltpu.make_async_remote_copy(
                src_ref=send1.at[target], dst_ref=recv1.at[r], send_sem=a_send.at[slot],
                recv_sem=a_recv.at[slot] if d == 0 else a_recv.at[2 * d + r % 2],
                device_id=(target, c), device_id_type=MESH,
            )
            copy.start()
            first_copies.append(copy)
    stay1 = pltpu.make_async_copy(send1.at[r], recv1.at[r], l_sem.at[0])
    stay1.start()

    for t in range(chips):
        slot = t * pair + lax.broadcasted_iota(jnp.int32, (pair, 4 * slab), 0)
        column = lax.broadcasted_iota(jnp.int32, (pair, 4 * slab), 1)
        within = slot % slab
        freq = (slot // slab) * half + within % half
        odd = within >= half
        nyquist = odd & (freq == 0)
        high = min(group_len - slab * (t + 1), group_len - pair)
        direct = (column == freq - slab * t) & ~nyquist & (column < slab)
        mirror = (column - slab + high == group_len - freq) & (freq > 0)
        mirror = mirror & (column >= slab) & (column < 3 * slab)
        middle = nyquist & (column == 3 * slab)
        signed = jnp.where(odd, -1.0, 1.0)
        fold_ref[t] = jnp.where(direct, signed, jnp.where(mirror | middle, 1.0, 0.0)).astype(BF16)

    w_copy.wait()
    wide = 256
    pieces = out_width // wide

    def fold_step(i, carry):
        base = pl.multiple_of((i // pieces) * group_len, group_len)
        cols = pl.ds(pl.multiple_of((i % pieces) * wide, wide), wide)
        for t in range(chips):
            high = min(group_len - slab * (t + 1), group_len - pair)
            taken = [w_ref[pl.ds(base + slab * t, slab), cols], w_ref[pl.ds(base + high, pair), cols]]
            if t == 0:
                taken.append(w_ref[pl.ds(base + group_len // 2, slab), cols])
            depth = slab * (4 if t == 0 else 3)
            folded[pl.ds(base + pair * t, pair), cols] = jnp.dot(
                fold_ref[t, :, :depth], jnp.concatenate(taken, 0), preferred_element_type=F32
            ).astype(BF16)
        return carry

    lax.fori_loop(0, col_count * pieces, fold_step, 0)

    def arrived(ref, semaphore):
        pltpu.make_async_remote_copy(
            src_ref=ref, dst_ref=ref, send_sem=l_sem.at[0], recv_sem=semaphore,
            device_id=(other, c), device_id_type=MESH,
        ).wait_recv()

    def block_of(d, i):
        return 2 * lax.rem(z - d + chips, chips) + i

    stay1.wait()
    twist_copy.wait()
    low_copy.wait()
    arrived(recv1.at[other], a_recv.at[0])
    for d in range(1, chips):
        for i in range(2):
            arrived(recv1.at[block_of(d, i)], a_recv.at[2 * d + i])
    tile = 32
    lane = lax.broadcasted_iota(jnp.int32, (tile, slab), 1)
    sine = (lane > half) | ((lane == half) & (r > 0))

    def turn_step(i, carry):
        rows = pl.ds(pl.multiple_of(i * tile, tile), tile)
        below = pl.ds(pl.multiple_of(block_len + i * tile, tile), tile)
        blocks = [recv1[a, rows, :].astype(F32) for a in range(row_count)]
        middle = row_count // 2
        even = [blocks[a] + blocks[row_count - a] for a in range(1, middle)]
        odd = [blocks[a] - blocks[row_count - a] for a in range(1, middle)]
        ends = (blocks[0] + blocks[middle], blocks[0] - blocks[middle])
        twist = twist_ref[rows, :]
        for q in range(middle + 1):
            real = ends[q % 2]
            imag = None
            for a in range(1, middle):
                angle = 2 * math.pi * (a * q % row_count) / row_count
                cosine, sinus = round(math.cos(angle), 12), round(math.sin(angle), 12)
                if cosine:
                    real = real + even[a - 1] * cosine
                if sinus:
                    term = odd[a - 1] * -sinus
                    imag = term if imag is None else imag + term
            for k, sign in ((q, 1.0), (row_count - q, -1.0)):
                if k == row_count or (sign < 0 and k == q):
                    continue
                cosine, sinus = twist[:, k : k + 1], twist[:, row_count + k : row_count + k + 1]
                if imag is None:
                    turned_real, turned_imag = real * cosine, -(real * sinus)
                else:
                    turned_real = real * cosine + imag * (sinus * sign)
                    turned_imag = imag * (cosine * sign) - real * sinus
                cols = pl.ds(k * slab, slab)
                stacked[rows, cols] = jnp.where(sine, -turned_imag, turned_real).astype(BF16)
                stacked[below, cols] = jnp.where(sine, turned_real, turned_imag).astype(BF16)
        return carry

    lax.fori_loop(0, block_len // tile, turn_step, 0)

    def lanes_of(index):
        return pl.ds(pl.multiple_of(index * slab, slab), slab)

    sends = []

    def share(origin, source, block, target, out_slot, in_slot):
        copy = pltpu.make_async_remote_copy(
            src_ref=source, dst_ref=lhs.at[origin, :, :, lanes_of(block)],
            send_sem=g_send.at[out_slot], recv_sem=g_recv.at[in_slot],
            device_id=(r, target), device_id_type=MESH,
        )
        copy.start()
        sends.append(copy)
        return copy

    def held(origin, block):
        return lhs.at[origin, :, :, lanes_of(block)]

    count = row_count
    from_x, from_y, from_far = [], [], []

    def offer(n, source, block):
        from_x.append(share(c, source, block, x_next, n, n))
        from_y.append(share(c, source, block, y_next, count + n, count + n))

    second_copies = []
    stay2 = pltpu.make_async_copy(send2.at[r], held(c, r), l_sem.at[1])
    for d in [0] + far_first[:-1]:
        chip = lax.rem(z + d, chips)
        lows = jnp.dot(
            low_ref[pl.ds(pl.multiple_of(chip * 2 * part, 2 * part), 2 * part), :], stacked[...],
            preferred_element_type=F32,
        ).astype(BF16)
        for i in range(2):
            for q in range(row_count):
                send2[2 * chip + i, q] = lows[i * part : (i + 1) * part, q * slab : (q + 1) * slab]
        for target, slot in ([(2 * chip, 2 * d), (2 * chip + 1, 2 * d + 1)] if d else [(other, 0)]):
            copy = pltpu.make_async_remote_copy(
                src_ref=send2.at[target], dst_ref=held(c, r),
                send_sem=b_send.at[slot],
                recv_sem=b_recv.at[slot] if d == 0 else b_recv.at[2 * d + r % 2],
                device_id=(target, c), device_id_type=MESH,
            )
            copy.start()
            second_copies.append(copy)
        if d == 0:
            offer(0, send2.at[r], r)
            stay2.start()

    near_first = sorted(range(chips), key=lambda d: min(d, chips - d))
    pairs = [lax.rem(z - d + chips, chips) for d in near_first]
    order = [(None, r), (0, other)]
    for d in near_first[1:]:
        order += [(2 * d + i, block_of(d, i)) for i in range(2)]

    def multiply(origin, m, first=False, last=False):
        base = pl.multiple_of(origin * group_len + pairs[m] * pair, pair)
        taken = pl.ds(pl.multiple_of(pairs[m] * pair, pair), pair)

        def step(i, carry):
            cols = pl.ds(pl.multiple_of(i * wide, wide), wide)
            left = lhs[origin, :, :, taken].reshape(block_len, pair)
            value = jnp.dot(left, folded[pl.ds(base, pair), cols], preferred_element_type=F32)
            if not first:
                value = acc[:, cols] + value
            if not last:
                acc[:, cols] = value
            else:
                for q in range(row_count):
                    for j in range(wide // 128):
                        spread[j, pl.ds(q, part, stride=row_count), :] = value[
                            q * part : (q + 1) * part, j * 128 : (j + 1) * 128
                        ]
                for j in range(wide // 128):
                    at = pl.ds(pl.multiple_of(i * wide + j * 128, 128), 128)
                    out_ref[:, at] = spread[j].astype(BF16)
            return carry

        lax.fori_loop(0, pieces, step, 0)

    def own_part(m):
        if m == 0:
            stay2.wait()
        multiply(c, m, first=m == 0)

    def x_part(m):
        from_x[2 * m + 1].wait_recv()
        multiply(x_next, m)

    def y_part(m):
        from_y[2 * m].wait_recv()
        multiply(y_next, m)

    def far_part(m):
        from_far[2 * m].wait_recv()
        from_far[2 * m + 1].wait_recv()
        multiply(diagonal, m, last=m == chips - 1)

    for n in range(1, count + 1):
        if n < count:
            slot, block = order[n]
            arrived(held(c, block), b_recv.at[slot])
            offer(n, held(c, block), block)
        _, block = order[n - 1]
        slot = 2 * count + n - 1
        if n % 2:
            from_x[n - 1].wait_recv()
            from_far.append(share(x_next, held(x_next, block), block, y_next, slot, slot))
        else:
            from_y[n - 1].wait_recv()
            from_far.append(share(y_next, held(y_next, block), block, x_next, slot, slot))
        m = n // 2
        if n % 2:
            own_part(m)
            if m:
                x_part(m - 1)
        elif 2 <= m < chips:
            y_part(m - 2)
            if m >= 3:
                far_part(m - 3)
    y_part(chips - 2)
    for m in range(max(chips - 3, 0), chips - 2):
        far_part(m)
    x_part(chips - 1)
    y_part(chips - 1)
    far_part(chips - 2)
    far_part(chips - 1)

    for copy in sum_copies + first_copies + second_copies + sends:
        copy.wait_send()


def on_device_fused(tokens, norm_gain, out_weight):
    row_count = lax.axis_size("row")
    col_count = lax.axis_size("col")
    block_len, group_len = tokens.shape
    out_width = out_weight.shape[1]
    slab = group_len // row_count
    part = block_len // row_count
    chan_table, low_table, twist_cos, twist_sin = host_tables(group_len, row_count, block_len)
    twist = np.zeros((block_len, 128), np.float32)
    twist[:, :row_count] = twist_cos.T
    twist[:, row_count : 2 * row_count] = twist_sin.T
    vmem = pl.BlockSpec(memory_space=pltpu.VMEM)
    dma = pltpu.SemaphoreType.DMA
    return pl.pallas_call(
        functools.partial(fused_kernel, (row_count, col_count)),
        out_shape=jax.ShapeDtypeStruct((block_len, out_width), BF16),
        in_specs=[vmem] * 2 + [pl.BlockSpec(memory_space=pl.ANY)] * 4,
        out_specs=vmem,
        scratch_shapes=[
            pltpu.VMEM(chan_table.shape, BF16),
            pltpu.VMEM(low_table.shape, BF16),
            pltpu.VMEM(twist.shape, F32),
            pltpu.VMEM(out_weight.shape, BF16),
            pltpu.VMEM((row_count // 2, 2 * slab, 4 * slab), BF16),
            pltpu.VMEM(out_weight.shape, BF16),
            pltpu.VMEM((row_count, block_len, slab), BF16),
            pltpu.VMEM((row_count, block_len, slab), BF16),
            pltpu.VMEM((col_count, 8, block_len), F32),
            pltpu.VMEM((2 * block_len, row_count * slab), BF16),
            pltpu.VMEM((row_count, row_count, part, slab), BF16),
            pltpu.VMEM((col_count, row_count, part, group_len), BF16),
            pltpu.VMEM((block_len, out_width), F32),
            pltpu.VMEM((2, block_len, 128), F32),
            dma, dma((col_count - 1,)), dma((col_count - 1,)),
            dma((row_count,)), dma((row_count,)), dma((row_count,)), dma((row_count,)),
            dma((3 * row_count,)), dma((3 * row_count,)), dma((5,)),
        ],
        compiler_params=pltpu.CompilerParams(
            collective_id=0, has_side_effects=True, vmem_limit_bytes=60 * 1024 * 1024
        ),
    )(
        tokens, norm_gain[None, :], jnp.asarray(chan_table, BF16), jnp.asarray(low_table, BF16),
        jnp.asarray(twist), out_weight,
    )


def on_device(tokens, norm_gain, out_weight):
    row_count = lax.axis_size("row")
    col_count = lax.axis_size("col")
    block_len, local_width = tokens.shape
    full_width = local_width * col_count
    group_len = full_width // GROUPS
    share_len = block_len // col_count
    seq_len = block_len * row_count
    slab_len = full_width // row_count
    col_index = lax.axis_index("col")
    chan_idx = jnp.arange(group_len, dtype=jnp.int32)
    cosines, sines = phases(chan_idx, chan_idx, group_len)
    chan_table = jnp.concatenate([cosines, sines], axis=1) / math.sqrt(group_len)
    table_parts = split_table(chan_table)
    arranged = tokens.reshape(col_count, share_len, local_width)
    portion = lax.all_to_all(arranged, "col", split_axis=0, concat_axis=2, tiled=True)
    item_count = portion.shape[1]
    values = portion.astype(jnp.float32)
    inv_rms = lax.rsqrt(jnp.mean(values * values, axis=-1, keepdims=True) + EPSILON)
    normed = lax.optimization_barrier((values * inv_rms * norm_gain).astype(jnp.bfloat16))
    grouped = normed.reshape(item_count, GROUPS, group_len)
    result = jnp.einsum("pgm,mj->pgj", grouped, table_parts[0], preferred_element_type=jnp.float32)
    result = result + jnp.einsum(
        "pgm,mj->pgj", grouped, table_parts[1], preferred_element_type=jnp.float32
    )
    result = result + jnp.einsum(
        "pgm,mj->pgj", grouped, table_parts[2], preferred_element_type=jnp.float32
    )
    high_idx = jnp.arange(row_count, dtype=jnp.int32)
    high_cos, high_sin = phases(high_idx, high_idx, row_count)
    high_table = jnp.concatenate(
        [jnp.concatenate([high_cos, -high_sin], 1), jnp.concatenate([-high_sin, -high_cos], 1)], 0
    )
    parts = (
        lax.all_to_all(
            result[..., :group_len].reshape(1, item_count, full_width),
            "row",
            split_axis=2,
            concat_axis=0,
            tiled=True,
        ),
        lax.all_to_all(
            result[..., group_len:].reshape(1, item_count, full_width),
            "row",
            split_axis=2,
            concat_axis=0,
            tiled=True,
        ),
    )
    item_count = parts[0].shape[1]
    stacked = jnp.concatenate(parts, 0).reshape(2 * row_count, item_count * slab_len)
    result = jnp.dot(high_table, stacked, precision=PRECISE)
    real_part = result[:row_count].reshape(row_count, item_count, slab_len)
    imag_part = result[row_count:].reshape(row_count, item_count, slab_len)
    local_pos = col_index * share_len + jnp.arange(share_len, dtype=jnp.int32)
    twist_cos, twist_sin = phases(high_idx, local_pos, seq_len)
    twist_cos = twist_cos[:, :, None]
    twist_sin = twist_sin[:, :, None]
    turned_real = real_part * twist_cos + imag_part * twist_sin
    turned_imag = imag_part * twist_cos - real_part * twist_sin
    low_idx = jnp.arange(block_len, dtype=jnp.int32)
    low_cos, low_sin = phases(low_idx, low_idx, block_len)
    low_cos = low_cos / math.sqrt(seq_len)
    low_sin = low_sin / math.sqrt(seq_len)
    low_table = jnp.concatenate([low_cos, low_sin], 1)
    stacked = jnp.concatenate(
        (
            lax.all_to_all(turned_real, "col", split_axis=0, concat_axis=1, tiled=True),
            lax.all_to_all(turned_imag, "col", split_axis=0, concat_axis=1, tiled=True),
        ),
        1,
    )
    finished = (jnp.einsum("ks,asc->akc", low_table, stacked, precision=PRECISE),)[0]
    spectrum = finished.astype(jnp.bfloat16)
    returned = lax.all_to_all(spectrum, "row", split_axis=1, concat_axis=2, tiled=True)
    mapped = jnp.einsum(
        "akd,de->kae",
        lax.all_gather(returned, "col", axis=0, tiled=True),
        out_weight,
        preferred_element_type=jnp.float32,
    )
    return mapped.astype(jnp.bfloat16).reshape(block_len, local_width)


def solution(mesh):
    def body(tokens, norm_gain, out_weight):
        whole_groups = tokens.shape[1] * GROUPS == out_weight.shape[0]
        slab = tokens.shape[1] // mesh.shape["row"]
        program = on_device_folded if whole_groups else on_device
        if whole_groups and slab == 128 and mesh.shape["col"] == 4 and mesh.shape["row"] == 8:
            program = on_device_fused
        return program(tokens, norm_gain, out_weight)

    placed = (P("row", "col"), P(), P(None, "col"))
    return jax.shard_map(
        body, mesh=mesh, in_specs=placed, out_specs=P("row", "col"), check_vma=False
    )
```

```python
import functools
import math

import numpy as np

import jax
import jax.numpy as jnp
from jax import lax
from jax.experimental import pallas as pl
from jax.experimental.pallas import tpu as pltpu
from jax.sharding import PartitionSpec as P

GROUPS = 4


EPSILON = 1e-06
PRECISE = lax.Precision.HIGHEST


def phases(left_idx, right_idx, period):
    product = left_idx[:, None] * right_idx[None, :] % period
    angles = product.astype(jnp.float32) * (2.0 * math.pi / period)
    return (jnp.cos(angles), jnp.sin(angles))


def split_table(table):
    table_high = table.astype(jnp.bfloat16)
    remainder = table - table_high.astype(jnp.float32)
    table_middle = remainder.astype(jnp.bfloat16)
    table_low = (remainder - table_middle.astype(jnp.float32)).astype(jnp.bfloat16)
    return (table_high, table_middle, table_low)


def host_tables(group_len, row_count, block_len):
    seq_len = block_len * row_count
    half = group_len // 2 // row_count
    slot = np.arange(group_len)
    freq = (slot // (2 * half)) * half + slot % half
    odd = slot // half % 2 == 1
    nyquist = odd & (freq == 0)
    sine = odd & ~nyquist
    freq = np.where(nyquist, group_len // 2, freq)
    chan = np.arange(group_len)
    angle = 2 * np.pi * (chan[:, None] * freq[None, :] % group_len) / group_len
    chan_table = np.where(sine[None, :], np.sin(angle), np.cos(angle)) / np.sqrt(group_len)
    low = np.arange(block_len)
    angle = 2 * np.pi * (low[:, None] * low[None, :] % block_len) / block_len
    low_table = np.concatenate([np.cos(angle), np.sin(angle)], 1) / np.sqrt(seq_len)
    high = np.arange(row_count)
    angle = 2 * np.pi * (high[:, None] * low[None, :] % seq_len) / seq_len
    return chan_table, low_table, np.cos(angle), np.sin(angle)


def slot_facts(slot, group_len, row_count):
    half = group_len // 2 // row_count
    freq = (slot // (2 * half)) * half + slot % half
    odd = slot // half % 2 == 1
    nyquist = odd & (freq == 0)
    return jnp.where(nyquist, group_len // 2, freq), odd & ~nyquist


def folding(group_len, row_count):
    freq, sine = slot_facts(jnp.arange(group_len, dtype=jnp.int32), group_len, row_count)
    chan = jnp.arange(group_len, dtype=jnp.int32)[None, :]
    direct = chan == freq[:, None]
    mirror = chan == ((group_len - freq) % group_len)[:, None]
    signed = jnp.where(sine[:, None], -1.0, 1.0)
    return jnp.where(direct, signed, jnp.where(mirror, 1.0, 0.0)).astype(jnp.bfloat16)


def on_device_folded(tokens, norm_gain, out_weight):
    row_count = lax.axis_size("row")
    col_count = lax.axis_size("col")
    block_len, group_len = tokens.shape
    full_width = group_len * col_count
    slab = group_len // row_count
    out_width = out_weight.shape[1]
    chan_table, low_table, twist_cos, twist_sin = host_tables(group_len, row_count, block_len)
    chan_table = jnp.asarray(chan_table, jnp.bfloat16)
    low_table = jnp.asarray(low_table, jnp.bfloat16)
    twist_cos = jnp.asarray(twist_cos, jnp.float32)[:, :, None]
    twist_sin = jnp.asarray(twist_sin, jnp.float32)[:, :, None]
    values = tokens.astype(jnp.float32)
    total = lax.psum(jnp.sum(values * values, axis=-1), "col")
    inv_rms = lax.rsqrt(total / full_width + EPSILON)[:, None]
    gain = lax.dynamic_slice_in_dim(norm_gain, lax.axis_index("col") * group_len, group_len)
    normed = (values * inv_rms * gain).astype(jnp.bfloat16)
    chans = jnp.dot(normed, chan_table, preferred_element_type=jnp.float32).astype(jnp.bfloat16)
    moved = lax.all_to_all(chans, "row", split_axis=1, concat_axis=0, tiled=True)
    blocks = moved.reshape(row_count, block_len, slab).astype(jnp.float32)
    _, sine = slot_facts(
        lax.axis_index("row") * slab + jnp.arange(slab, dtype=jnp.int32), group_len, row_count
    )
    tops, bottoms = [], []
    for q in range(row_count):
        real, imag = 0.0, 0.0
        for a in range(row_count):
            angle = 2 * math.pi * (a * q % row_count) / row_count
            real = real + blocks[a] * round(math.cos(angle), 12)
            imag = imag - blocks[a] * round(math.sin(angle), 12)
        turned_real = real * twist_cos[q] + imag * twist_sin[q]
        turned_imag = imag * twist_cos[q] - real * twist_sin[q]
        tops.append(jnp.where(sine, -turned_imag, turned_real).astype(jnp.bfloat16))
        bottoms.append(jnp.where(sine, turned_real, turned_imag).astype(jnp.bfloat16))
    stacked = jnp.concatenate([jnp.concatenate(tops, 1), jnp.concatenate(bottoms, 1)], 0)
    lows = jnp.dot(low_table, stacked, preferred_element_type=jnp.float32).astype(jnp.bfloat16)
    back = lax.all_to_all(
        lows.reshape(row_count, block_len // row_count, row_count * slab),
        "row", split_axis=0, concat_axis=0, tiled=True,
    )
    gathered = lax.all_gather(back, "col", axis=0, tiled=False)
    fold = folding(group_len, row_count)
    folded = jnp.einsum(
        "sm,gme->gse", fold, out_weight.reshape(col_count, group_len, out_width),
        preferred_element_type=jnp.float32,
    ).astype(jnp.bfloat16)
    mapped = jnp.einsum(
        "gspql,gsle->pqe",
        gathered.reshape(col_count, row_count, block_len // row_count, row_count, slab),
        folded.reshape(col_count, row_count, slab, out_width),
        preferred_element_type=jnp.float32,
    )
    return mapped.astype(jnp.bfloat16).reshape(block_len, out_width)


MESH = pl.DeviceIdType.MESH
F32 = jnp.float32
BF16 = jnp.bfloat16


def fused_kernel(
    dims, x_ref, gain_ref, table_hbm, low_hbm, twist_hbm, w_hbm, out_ref,
    table_ref, low_ref, twist_in, twist_ref, w_ref, fold_ref, folded, send1, recv1, sums, stacked, send2, lhs, acc,
    w_sem, s_send, s_recv, a_send, a_recv, b_send, b_recv, g_send, g_recv, l_sem,
):
    row_count, col_count = dims
    block_len, group_len = x_ref.shape
    full_width = group_len * col_count
    slab = group_len // row_count
    half = slab // 2
    pair = 2 * slab
    chips = row_count // 2
    part = block_len // row_count
    out_width = out_ref.shape[2]
    r = lax.axis_index("row")
    c = lax.axis_index("col")
    z = r // 2
    other = 2 * z + 1 - r % 2
    x_next = 2 * (c // 2) + 1 - c % 2
    y_next = 2 * (1 - c // 2) + c % 2
    diagonal = 2 * (1 - c // 2) + 1 - c % 2
    col_peers = (x_next, y_next, diagonal)
    table_copy = pltpu.make_async_copy(table_hbm, table_ref, l_sem.at[2])
    w_copy = pltpu.make_async_copy(w_hbm, w_ref, w_sem)
    low_copy = pltpu.make_async_copy(low_hbm, low_ref, l_sem.at[3])
    twist_copy = pltpu.make_async_copy(twist_hbm, twist_in, l_sem.at[4])
    for copy in (table_copy, w_copy, low_copy, twist_copy):
        copy.start()

    barrier = pltpu.get_barrier_semaphore()
    for step in range(1, row_count):
        pl.semaphore_signal(
            barrier, inc=1, device_id=(lax.rem(r + step, row_count), c), device_id_type=MESH
        )
    for peer in col_peers:
        pl.semaphore_signal(barrier, inc=1, device_id=(r, peer), device_id_type=MESH)
    values = x_ref[...].astype(F32)
    squares = values * values
    top = squares.astype(BF16)
    rest = (squares - top.astype(F32)).astype(BF16)
    ones = jnp.ones((16, group_len), BF16)
    lanes = (((1,), (1,)), ((), ()))
    own = lax.dot_general(ones, top, lanes, preferred_element_type=F32)
    own = own + lax.dot_general(ones, rest, lanes, preferred_element_type=F32)
    sums[c] = own[:8]
    pl.semaphore_wait(barrier, row_count + col_count - 2)
    sum_copies = []
    for k, peer in enumerate(col_peers):
        copy = pltpu.make_async_remote_copy(
            src_ref=sums.at[c], dst_ref=sums.at[c], send_sem=s_send.at[k], recv_sem=s_recv.at[k],
            device_id=(r, peer), device_id_type=MESH,
        )
        copy.start()
        sum_copies.append(copy)

    gain = gain_ref[:, pl.ds(pl.multiple_of(c * group_len, group_len), group_len)]
    scaled = (values * gain).astype(BF16)
    far_first = sorted(range(chips), key=lambda d: -min(d, chips - d))
    first_copies = []
    inv = None
    table_copy.wait()
    for d in far_first:
        chip = lax.rem(z + d, chips)
        product = jnp.dot(
            scaled, table_ref[:, pl.ds(pl.multiple_of(chip * pair, pair), pair)],
            preferred_element_type=F32,
        )
        if inv is None:
            for copy in sum_copies:
                copy.wait_recv()
            total = sums[0, :1, :]
            for k in range(1, col_count):
                total = total + sums[k, :1, :]
            inv = lax.rsqrt(total / full_width + EPSILON)
            inv = jnp.transpose(jnp.broadcast_to(inv, (128, block_len)))
        send1[2 * chip] = (product[:, :slab] * inv).astype(BF16)
        send1[2 * chip + 1] = (product[:, slab:] * inv).astype(BF16)
        for target, slot in ([(2 * chip, 2 * d), (2 * chip + 1, 2 * d + 1)] if d else [(other, 0)]):
            copy = pltpu.make_async_remote_copy(
                src_ref=send1.at[target], dst_ref=recv1.at[r], send_sem=a_send.at[slot],
                recv_sem=a_recv.at[slot] if d == 0 else a_recv.at[2 * d + r % 2],
                device_id=(target, c), device_id_type=MESH,
            )
            copy.start()
            first_copies.append(copy)
    stay1 = pltpu.make_async_copy(send1.at[r], recv1.at[r], l_sem.at[0])
    stay1.start()

    for t in range(chips):
        slot = t * pair + lax.broadcasted_iota(jnp.int32, (pair, 4 * slab), 0)
        column = lax.broadcasted_iota(jnp.int32, (pair, 4 * slab), 1)
        within = slot % slab
        freq = (slot // slab) * half + within % half
        odd = within >= half
        nyquist = odd & (freq == 0)
        high = min(group_len - slab * (t + 1), group_len - pair)
        direct = (column == freq - slab * t) & ~nyquist & (column < slab)
        mirror = (column - slab + high == group_len - freq) & (freq > 0)
        mirror = mirror & (column >= slab) & (column < 3 * slab)
        middle = nyquist & (column == 3 * slab)
        signed = jnp.where(odd, -1.0, 1.0)
        fold_ref[t] = jnp.where(direct, signed, jnp.where(mirror | middle, 1.0, 0.0)).astype(BF16)

    twist_copy.wait()
    filler = jnp.zeros((128 - 2 * row_count, block_len), F32)
    twist_ref[...] = jnp.transpose(jnp.concatenate([twist_in[...], filler], 0))
    w_copy.wait()
    wide = 256
    pieces = out_width // wide

    def fold_step(i, carry):
        base = pl.multiple_of((i // pieces) * group_len, group_len)
        cols = pl.ds(pl.multiple_of((i % pieces) * wide, wide), wide)
        for t in range(chips):
            high = min(group_len - slab * (t + 1), group_len - pair)
            taken = [w_ref[pl.ds(base + slab * t, slab), cols], w_ref[pl.ds(base + high, pair), cols]]
            if t == 0:
                taken.append(w_ref[pl.ds(base + group_len // 2, slab), cols])
            depth = slab * (4 if t == 0 else 3)
            folded[pl.ds(base + pair * t, pair), cols] = jnp.dot(
                fold_ref[t, :, :depth], jnp.concatenate(taken, 0), preferred_element_type=F32
            ).astype(BF16)
        return carry

    lax.fori_loop(0, col_count * pieces, fold_step, 0)

    def arrived(ref, semaphore):
        pltpu.make_async_remote_copy(
            src_ref=ref, dst_ref=ref, send_sem=l_sem.at[0], recv_sem=semaphore,
            device_id=(other, c), device_id_type=MESH,
        ).wait_recv()

    def block_of(d, i):
        return 2 * lax.rem(z - d + chips, chips) + i

    stay1.wait()
    low_copy.wait()
    arrived(recv1.at[other], a_recv.at[0])
    for d in range(1, chips):
        for i in range(2):
            arrived(recv1.at[block_of(d, i)], a_recv.at[2 * d + i])
    tile = 32
    lane = lax.broadcasted_iota(jnp.int32, (tile, slab), 1)
    sine = (lane > half) | ((lane == half) & (r > 0))

    def turn_step(i, carry):
        rows = pl.ds(pl.multiple_of(i * tile, tile), tile)
        below = pl.ds(pl.multiple_of(block_len + i * tile, tile), tile)
        blocks = [recv1[a, rows, :].astype(F32) for a in range(row_count)]
        middle = row_count // 2
        even = [blocks[a] + blocks[row_count - a] for a in range(1, middle)]
        odd = [blocks[a] - blocks[row_count - a] for a in range(1, middle)]
        ends = (blocks[0] + blocks[middle], blocks[0] - blocks[middle])
        twist = twist_ref[rows, :]
        for q in range(middle + 1):
            real = ends[q % 2]
            imag = None
            for a in range(1, middle):
                angle = 2 * math.pi * (a * q % row_count) / row_count
                cosine, sinus = round(math.cos(angle), 12), round(math.sin(angle), 12)
                if cosine:
                    real = real + even[a - 1] * cosine
                if sinus:
                    term = odd[a - 1] * -sinus
                    imag = term if imag is None else imag + term
            for k, sign in ((q, 1.0), (row_count - q, -1.0)):
                if k == row_count or (sign < 0 and k == q):
                    continue
                cosine, sinus = twist[:, k : k + 1], twist[:, row_count + k : row_count + k + 1]
                if imag is None:
                    turned_real, turned_imag = real * cosine, -(real * sinus)
                else:
                    turned_real = real * cosine + imag * (sinus * sign)
                    turned_imag = imag * (cosine * sign) - real * sinus
                cols = pl.ds(k * slab, slab)
                stacked[rows, cols] = jnp.where(sine, -turned_imag, turned_real).astype(BF16)
                stacked[below, cols] = jnp.where(sine, turned_real, turned_imag).astype(BF16)
        return carry

    lax.fori_loop(0, block_len // tile, turn_step, 0)

    def lanes_of(index):
        return pl.ds(pl.multiple_of(index * slab, slab), slab)

    sends = []

    def share(origin, source, block, target, out_slot, in_slot):
        copy = pltpu.make_async_remote_copy(
            src_ref=source, dst_ref=lhs.at[origin, :, :, lanes_of(block)],
            send_sem=g_send.at[out_slot], recv_sem=g_recv.at[in_slot],
            device_id=(r, target), device_id_type=MESH,
        )
        copy.start()
        sends.append(copy)
        return copy

    def held(origin, block):
        return lhs.at[origin, :, :, lanes_of(block)]

    count = row_count
    from_x, from_y, from_far = [], [], []

    def offer(n, source, block):
        from_x.append(share(c, source, block, x_next, n, n))
        from_y.append(share(c, source, block, y_next, count + n, count + n))

    second_copies = []
    stay2 = pltpu.make_async_copy(send2.at[r], held(c, r), l_sem.at[1])
    for d in [0] + far_first[:-1]:
        chip = lax.rem(z + d, chips)
        lows = jnp.dot(
            low_ref[pl.ds(pl.multiple_of(chip * 2 * part, 2 * part), 2 * part), :], stacked[...],
            preferred_element_type=F32,
        ).astype(BF16)
        for i in range(2):
            for q in range(row_count):
                send2[2 * chip + i, q] = lows[i * part : (i + 1) * part, q * slab : (q + 1) * slab]
        for target, slot in ([(2 * chip, 2 * d), (2 * chip + 1, 2 * d + 1)] if d else [(other, 0)]):
            copy = pltpu.make_async_remote_copy(
                src_ref=send2.at[target], dst_ref=held(c, r),
                send_sem=b_send.at[slot],
                recv_sem=b_recv.at[slot] if d == 0 else b_recv.at[2 * d + r % 2],
                device_id=(target, c), device_id_type=MESH,
            )
            copy.start()
            second_copies.append(copy)
        if d == 0:
            offer(0, send2.at[r], r)
            stay2.start()

    near_first = sorted(range(chips), key=lambda d: min(d, chips - d))
    pairs = [lax.rem(z - d + chips, chips) for d in near_first]
    order = [(None, r), (0, other)]
    for d in near_first[1:]:
        order += [(2 * d + i, block_of(d, i)) for i in range(2)]

    def multiply(origin, m, first=False, last=False):
        base = pl.multiple_of(origin * group_len + pairs[m] * pair, pair)
        taken = pl.ds(pl.multiple_of(pairs[m] * pair, pair), pair)

        def step(i, carry):
            cols = pl.ds(pl.multiple_of(i * wide, wide), wide)
            left = lhs[origin, :, :, taken].reshape(block_len, pair)
            value = jnp.dot(left, folded[pl.ds(base, pair), cols], preferred_element_type=F32)
            if not first:
                value = acc[:, cols] + value
            if not last:
                acc[:, cols] = value
            else:
                out_ref[:, :, cols] = value.astype(BF16).reshape(row_count, part, wide)
            return carry

        lax.fori_loop(0, pieces, step, 0)

    def own_part(m):
        if m == 0:
            stay2.wait()
        multiply(c, m, first=m == 0)

    def x_part(m):
        from_x[2 * m + 1].wait_recv()
        multiply(x_next, m)

    def y_part(m):
        from_y[2 * m].wait_recv()
        multiply(y_next, m)

    def far_part(m):
        from_far[2 * m].wait_recv()
        from_far[2 * m + 1].wait_recv()
        multiply(diagonal, m, last=m == chips - 1)

    for n in range(1, count + 1):
        if n < count:
            slot, block = order[n]
            arrived(held(c, block), b_recv.at[slot])
            offer(n, held(c, block), block)
        _, block = order[n - 1]
        slot = 2 * count + n - 1
        if n % 2:
            from_x[n - 1].wait_recv()
            from_far.append(share(x_next, held(x_next, block), block, y_next, slot, slot))
        else:
            from_y[n - 1].wait_recv()
            from_far.append(share(y_next, held(y_next, block), block, x_next, slot, slot))
        m = n // 2
        if n % 2:
            own_part(m)
            if m:
                x_part(m - 1)
        elif 2 <= m < chips:
            y_part(m - 2)
            if m >= 3:
                far_part(m - 3)
    y_part(chips - 2)
    for m in range(max(chips - 3, 0), chips - 2):
        far_part(m)
    x_part(chips - 1)
    y_part(chips - 1)
    far_part(chips - 2)
    far_part(chips - 1)

    for copy in sum_copies + first_copies + second_copies + sends:
        copy.wait_send()


def on_device_fused(tokens, norm_gain, out_weight):
    row_count = lax.axis_size("row")
    col_count = lax.axis_size("col")
    block_len, group_len = tokens.shape
    out_width = out_weight.shape[1]
    slab = group_len // row_count
    part = block_len // row_count
    chan_table, low_table, twist_cos, twist_sin = host_tables(group_len, row_count, block_len)
    twist = np.concatenate([twist_cos, twist_sin], 0).astype(np.float32)
    vmem = pl.BlockSpec(memory_space=pltpu.VMEM)
    dma = pltpu.SemaphoreType.DMA
    mapped = pl.pallas_call(
        functools.partial(fused_kernel, (row_count, col_count)),
        out_shape=jax.ShapeDtypeStruct((row_count, part, out_width), BF16),
        in_specs=[vmem] * 2 + [pl.BlockSpec(memory_space=pl.ANY)] * 4,
        out_specs=vmem,
        scratch_shapes=[
            pltpu.VMEM(chan_table.shape, BF16),
            pltpu.VMEM(low_table.shape, BF16),
            pltpu.VMEM(twist.shape, F32),
            pltpu.VMEM((block_len, 128), F32),
            pltpu.VMEM(out_weight.shape, BF16),
            pltpu.VMEM((row_count // 2, 2 * slab, 4 * slab), BF16),
            pltpu.VMEM(out_weight.shape, BF16),
            pltpu.VMEM((row_count, block_len, slab), BF16),
            pltpu.VMEM((row_count, block_len, slab), BF16),
            pltpu.VMEM((col_count, 8, block_len), F32),
            pltpu.VMEM((2 * block_len, row_count * slab), BF16),
            pltpu.VMEM((row_count, row_count, part, slab), BF16),
            pltpu.VMEM((col_count, row_count, part, group_len), BF16),
            pltpu.VMEM((block_len, out_width), F32),
            dma, dma((col_count - 1,)), dma((col_count - 1,)),
            dma((row_count,)), dma((row_count,)), dma((row_count,)), dma((row_count,)),
            dma((3 * row_count,)), dma((3 * row_count,)), dma((5,)),
        ],
        compiler_params=pltpu.CompilerParams(
            collective_id=0, has_side_effects=True, vmem_limit_bytes=60 * 1024 * 1024
        ),
    )(
        tokens, norm_gain[None, :], jnp.asarray(chan_table, BF16), jnp.asarray(low_table, BF16),
        jnp.asarray(twist), out_weight,
    )
    return jnp.transpose(mapped, (1, 0, 2)).reshape(block_len, out_width)


def on_device(tokens, norm_gain, out_weight):
    row_count = lax.axis_size("row")
    col_count = lax.axis_size("col")
    block_len, local_width = tokens.shape
    full_width = local_width * col_count
    group_len = full_width // GROUPS
    share_len = block_len // col_count
    seq_len = block_len * row_count
    slab_len = full_width // row_count
    col_index = lax.axis_index("col")
    chan_idx = jnp.arange(group_len, dtype=jnp.int32)
    cosines, sines = phases(chan_idx, chan_idx, group_len)
    chan_table = jnp.concatenate([cosines, sines], axis=1) / math.sqrt(group_len)
    table_parts = split_table(chan_table)
    arranged = tokens.reshape(col_count, share_len, local_width)
    portion = lax.all_to_all(arranged, "col", split_axis=0, concat_axis=2, tiled=True)
    item_count = portion.shape[1]
    values = portion.astype(jnp.float32)
    inv_rms = lax.rsqrt(jnp.mean(values * values, axis=-1, keepdims=True) + EPSILON)
    normed = lax.optimization_barrier((values * inv_rms * norm_gain).astype(jnp.bfloat16))
    grouped = normed.reshape(item_count, GROUPS, group_len)
    result = jnp.einsum("pgm,mj->pgj", grouped, table_parts[0], preferred_element_type=jnp.float32)
    result = result + jnp.einsum(
        "pgm,mj->pgj", grouped, table_parts[1], preferred_element_type=jnp.float32
    )
    result = result + jnp.einsum(
        "pgm,mj->pgj", grouped, table_parts[2], preferred_element_type=jnp.float32
    )
    high_idx = jnp.arange(row_count, dtype=jnp.int32)
    high_cos, high_sin = phases(high_idx, high_idx, row_count)
    high_table = jnp.concatenate(
        [jnp.concatenate([high_cos, -high_sin], 1), jnp.concatenate([-high_sin, -high_cos], 1)], 0
    )
    parts = (
        lax.all_to_all(
            result[..., :group_len].reshape(1, item_count, full_width),
            "row",
            split_axis=2,
            concat_axis=0,
            tiled=True,
        ),
        lax.all_to_all(
            result[..., group_len:].reshape(1, item_count, full_width),
            "row",
            split_axis=2,
            concat_axis=0,
            tiled=True,
        ),
    )
    item_count = parts[0].shape[1]
    stacked = jnp.concatenate(parts, 0).reshape(2 * row_count, item_count * slab_len)
    result = jnp.dot(high_table, stacked, precision=PRECISE)
    real_part = result[:row_count].reshape(row_count, item_count, slab_len)
    imag_part = result[row_count:].reshape(row_count, item_count, slab_len)
    local_pos = col_index * share_len + jnp.arange(share_len, dtype=jnp.int32)
    twist_cos, twist_sin = phases(high_idx, local_pos, seq_len)
    twist_cos = twist_cos[:, :, None]
    twist_sin = twist_sin[:, :, None]
    turned_real = real_part * twist_cos + imag_part * twist_sin
    turned_imag = imag_part * twist_cos - real_part * twist_sin
    low_idx = jnp.arange(block_len, dtype=jnp.int32)
    low_cos, low_sin = phases(low_idx, low_idx, block_len)
    low_cos = low_cos / math.sqrt(seq_len)
    low_sin = low_sin / math.sqrt(seq_len)
    low_table = jnp.concatenate([low_cos, low_sin], 1)
    stacked = jnp.concatenate(
        (
            lax.all_to_all(turned_real, "col", split_axis=0, concat_axis=1, tiled=True),
            lax.all_to_all(turned_imag, "col", split_axis=0, concat_axis=1, tiled=True),
        ),
        1,
    )
    finished = (jnp.einsum("ks,asc->akc", low_table, stacked, precision=PRECISE),)[0]
    spectrum = finished.astype(jnp.bfloat16)
    returned = lax.all_to_all(spectrum, "row", split_axis=1, concat_axis=2, tiled=True)
    mapped = jnp.einsum(
        "akd,de->kae",
        lax.all_gather(returned, "col", axis=0, tiled=True),
        out_weight,
        preferred_element_type=jnp.float32,
    )
    return mapped.astype(jnp.bfloat16).reshape(block_len, local_width)


def solution(mesh):
    def body(tokens, norm_gain, out_weight):
        whole_groups = tokens.shape[1] * GROUPS == out_weight.shape[0]
        slab = tokens.shape[1] // mesh.shape["row"]
        program = on_device_folded if whole_groups else on_device
        if whole_groups and slab == 128 and mesh.shape["col"] == 4 and mesh.shape["row"] == 8:
            program = on_device_fused
        return program(tokens, norm_gain, out_weight)

    placed = (P("row", "col"), P(), P(None, "col"))
    return jax.shard_map(
        body, mesh=mesh, in_specs=placed, out_specs=P("row", "col"), check_vma=False
    )
```

```python
import functools
import math

import numpy as np

import jax
import jax.numpy as jnp
from jax import lax
from jax.experimental import pallas as pl
from jax.experimental.pallas import tpu as pltpu
from jax.sharding import PartitionSpec as P

GROUPS = 4


EPSILON = 1e-06
PRECISE = lax.Precision.HIGHEST


def phases(left_idx, right_idx, period):
    product = left_idx[:, None] * right_idx[None, :] % period
    angles = product.astype(jnp.float32) * (2.0 * math.pi / period)
    return (jnp.cos(angles), jnp.sin(angles))


def split_table(table):
    table_high = table.astype(jnp.bfloat16)
    remainder = table - table_high.astype(jnp.float32)
    table_middle = remainder.astype(jnp.bfloat16)
    table_low = (remainder - table_middle.astype(jnp.float32)).astype(jnp.bfloat16)
    return (table_high, table_middle, table_low)


def host_tables(group_len, row_count, block_len):
    seq_len = block_len * row_count
    half = group_len // 2 // row_count
    slot = np.arange(group_len)
    freq = (slot // (2 * half)) * half + slot % half
    odd = slot // half % 2 == 1
    nyquist = odd & (freq == 0)
    sine = odd & ~nyquist
    freq = np.where(nyquist, group_len // 2, freq)
    chan = np.arange(group_len)
    angle = 2 * np.pi * (chan[:, None] * freq[None, :] % group_len) / group_len
    chan_table = np.where(sine[None, :], np.sin(angle), np.cos(angle)) / np.sqrt(group_len)
    low = np.arange(block_len)
    angle = 2 * np.pi * (low[:, None] * low[None, :] % block_len) / block_len
    low_table = np.concatenate([np.cos(angle), np.sin(angle)], 1) / np.sqrt(seq_len)
    high = np.arange(row_count)
    angle = 2 * np.pi * (high[:, None] * low[None, :] % seq_len) / seq_len
    return chan_table, low_table, np.cos(angle), np.sin(angle)


def slot_facts(slot, group_len, row_count):
    half = group_len // 2 // row_count
    freq = (slot // (2 * half)) * half + slot % half
    odd = slot // half % 2 == 1
    nyquist = odd & (freq == 0)
    return jnp.where(nyquist, group_len // 2, freq), odd & ~nyquist


def folding(group_len, row_count):
    freq, sine = slot_facts(jnp.arange(group_len, dtype=jnp.int32), group_len, row_count)
    chan = jnp.arange(group_len, dtype=jnp.int32)[None, :]
    direct = chan == freq[:, None]
    mirror = chan == ((group_len - freq) % group_len)[:, None]
    signed = jnp.where(sine[:, None], -1.0, 1.0)
    return jnp.where(direct, signed, jnp.where(mirror, 1.0, 0.0)).astype(jnp.bfloat16)


def on_device_folded(tokens, norm_gain, out_weight):
    row_count = lax.axis_size("row")
    col_count = lax.axis_size("col")
    block_len, group_len = tokens.shape
    full_width = group_len * col_count
    slab = group_len // row_count
    out_width = out_weight.shape[1]
    chan_table, low_table, twist_cos, twist_sin = host_tables(group_len, row_count, block_len)
    chan_table = jnp.asarray(chan_table, jnp.bfloat16)
    low_table = jnp.asarray(low_table, jnp.bfloat16)
    twist_cos = jnp.asarray(twist_cos, jnp.float32)[:, :, None]
    twist_sin = jnp.asarray(twist_sin, jnp.float32)[:, :, None]
    values = tokens.astype(jnp.float32)
    total = lax.psum(jnp.sum(values * values, axis=-1), "col")
    inv_rms = lax.rsqrt(total / full_width + EPSILON)[:, None]
    gain = lax.dynamic_slice_in_dim(norm_gain, lax.axis_index("col") * group_len, group_len)
    normed = (values * inv_rms * gain).astype(jnp.bfloat16)
    chans = jnp.dot(normed, chan_table, preferred_element_type=jnp.float32).astype(jnp.bfloat16)
    moved = lax.all_to_all(chans, "row", split_axis=1, concat_axis=0, tiled=True)
    blocks = moved.reshape(row_count, block_len, slab).astype(jnp.float32)
    _, sine = slot_facts(
        lax.axis_index("row") * slab + jnp.arange(slab, dtype=jnp.int32), group_len, row_count
    )
    tops, bottoms = [], []
    for q in range(row_count):
        real, imag = 0.0, 0.0
        for a in range(row_count):
            angle = 2 * math.pi * (a * q % row_count) / row_count
            real = real + blocks[a] * round(math.cos(angle), 12)
            imag = imag - blocks[a] * round(math.sin(angle), 12)
        turned_real = real * twist_cos[q] + imag * twist_sin[q]
        turned_imag = imag * twist_cos[q] - real * twist_sin[q]
        tops.append(jnp.where(sine, -turned_imag, turned_real).astype(jnp.bfloat16))
        bottoms.append(jnp.where(sine, turned_real, turned_imag).astype(jnp.bfloat16))
    stacked = jnp.concatenate([jnp.concatenate(tops, 1), jnp.concatenate(bottoms, 1)], 0)
    lows = jnp.dot(low_table, stacked, preferred_element_type=jnp.float32).astype(jnp.bfloat16)
    back = lax.all_to_all(
        lows.reshape(row_count, block_len // row_count, row_count * slab),
        "row", split_axis=0, concat_axis=0, tiled=True,
    )
    gathered = lax.all_gather(back, "col", axis=0, tiled=False)
    fold = folding(group_len, row_count)
    folded = jnp.einsum(
        "sm,gme->gse", fold, out_weight.reshape(col_count, group_len, out_width),
        preferred_element_type=jnp.float32,
    ).astype(jnp.bfloat16)
    mapped = jnp.einsum(
        "gspql,gsle->pqe",
        gathered.reshape(col_count, row_count, block_len // row_count, row_count, slab),
        folded.reshape(col_count, row_count, slab, out_width),
        preferred_element_type=jnp.float32,
    )
    return mapped.astype(jnp.bfloat16).reshape(block_len, out_width)


MESH = pl.DeviceIdType.MESH
F32 = jnp.float32
BF16 = jnp.bfloat16


def fused_kernel(
    dims, x_ref, gain_ref, table_hbm, low_hbm, twist_hbm, w_hbm, out_ref,
    table_ref, low_ref, twist_in, twist_ref, w_ref, fold_ref, folded, send1, recv1, sums, stacked, send2, lhs, acc,
    w_sem, s_send, s_recv, a_send, a_recv, b_send, b_recv, g_send, g_recv, l_sem,
):
    row_count, col_count = dims
    block_len, group_len = x_ref.shape
    full_width = group_len * col_count
    slab = group_len // row_count
    half = slab // 2
    pair = 2 * slab
    chips = row_count // 2
    part = block_len // row_count
    out_width = out_ref.shape[2]
    r = lax.axis_index("row")
    c = lax.axis_index("col")
    z = r // 2
    other = 2 * z + 1 - r % 2
    x_next = 2 * (c // 2) + 1 - c % 2
    y_next = 2 * (1 - c // 2) + c % 2
    diagonal = 2 * (1 - c // 2) + 1 - c % 2
    col_peers = (x_next, y_next, diagonal)
    table_copy = pltpu.make_async_copy(table_hbm, table_ref, l_sem.at[2])
    w_copy = pltpu.make_async_copy(w_hbm, w_ref, w_sem)
    low_copy = pltpu.make_async_copy(low_hbm, low_ref, l_sem.at[3])
    twist_copy = pltpu.make_async_copy(twist_hbm, twist_in, l_sem.at[4])
    for copy in (table_copy, w_copy, low_copy, twist_copy):
        copy.start()

    barrier = pltpu.get_barrier_semaphore()
    for step in range(1, row_count):
        pl.semaphore_signal(
            barrier, inc=1, device_id=(lax.rem(r + step, row_count), c), device_id_type=MESH
        )
    for peer in col_peers:
        pl.semaphore_signal(barrier, inc=1, device_id=(r, peer), device_id_type=MESH)
    values = x_ref[...].astype(F32)
    squares = values * values
    top = squares.astype(BF16)
    rest = (squares - top.astype(F32)).astype(BF16)
    ones = jnp.ones((16, group_len), BF16)
    lanes = (((1,), (1,)), ((), ()))
    own = lax.dot_general(ones, top, lanes, preferred_element_type=F32)
    own = own + lax.dot_general(ones, rest, lanes, preferred_element_type=F32)
    sums[c] = own[:8]
    pl.semaphore_wait(barrier, row_count + col_count - 2)
    sum_copies = []
    for k, peer in enumerate(col_peers):
        copy = pltpu.make_async_remote_copy(
            src_ref=sums.at[c], dst_ref=sums.at[c], send_sem=s_send.at[k], recv_sem=s_recv.at[k],
            device_id=(r, peer), device_id_type=MESH,
        )
        copy.start()
        sum_copies.append(copy)

    gain = gain_ref[:, pl.ds(pl.multiple_of(c * group_len, group_len), group_len)]
    scaled = (values * gain).astype(BF16)
    far_first = sorted(range(chips), key=lambda d: -min(d, chips - d))
    first_copies = []
    inv = None
    table_copy.wait()
    for d in far_first:
        chip = lax.rem(z + d, chips)
        product = jnp.dot(
            scaled, table_ref[:, pl.ds(pl.multiple_of(chip * pair, pair), pair)],
            preferred_element_type=F32,
        )
        if inv is None:
            for copy in sum_copies:
                copy.wait_recv()
            total = sums[0, :1, :]
            for k in range(1, col_count):
                total = total + sums[k, :1, :]
            inv = lax.rsqrt(total / full_width + EPSILON)
            inv = jnp.transpose(jnp.broadcast_to(inv, (128, block_len)))
        send1[2 * chip] = (product[:, :slab] * inv).astype(BF16)
        send1[2 * chip + 1] = (product[:, slab:] * inv).astype(BF16)
        for target, slot in ([(2 * chip, 2 * d), (2 * chip + 1, 2 * d + 1)] if d else [(other, 0)]):
            copy = pltpu.make_async_remote_copy(
                src_ref=send1.at[target], dst_ref=recv1.at[r], send_sem=a_send.at[slot],
                recv_sem=a_recv.at[slot] if d == 0 else a_recv.at[2 * d + r % 2],
                device_id=(target, c), device_id_type=MESH,
            )
            copy.start()
            first_copies.append(copy)
    stay1 = pltpu.make_async_copy(send1.at[r], recv1.at[r], l_sem.at[0])
    stay1.start()

    for t in range(chips):
        slot = t * pair + lax.broadcasted_iota(jnp.int32, (pair, 4 * slab), 0)
        column = lax.broadcasted_iota(jnp.int32, (pair, 4 * slab), 1)
        within = slot % slab
        freq = (slot // slab) * half + within % half
        odd = within >= half
        nyquist = odd & (freq == 0)
        high = min(group_len - slab * (t + 1), group_len - pair)
        direct = (column == freq - slab * t) & ~nyquist & (column < slab)
        mirror = (column - slab + high == group_len - freq) & (freq > 0)
        mirror = mirror & (column >= slab) & (column < 3 * slab)
        middle = nyquist & (column == 3 * slab)
        signed = jnp.where(odd, -1.0, 1.0)
        fold_ref[t] = jnp.where(direct, signed, jnp.where(mirror | middle, 1.0, 0.0)).astype(BF16)

    twist_copy.wait()
    filler = jnp.zeros((128 - 2 * row_count, block_len), F32)
    twist_ref[...] = jnp.transpose(jnp.concatenate([twist_in[...], filler], 0))
    w_copy.wait()
    wide = 256
    pieces = out_width // wide

    def fold_step(i, carry):
        base = pl.multiple_of((i // pieces) * group_len, group_len)
        cols = pl.ds(pl.multiple_of((i % pieces) * wide, wide), wide)
        for t in range(chips):
            high = min(group_len - slab * (t + 1), group_len - pair)
            taken = [w_ref[pl.ds(base + slab * t, slab), cols], w_ref[pl.ds(base + high, pair), cols]]
            if t == 0:
                taken.append(w_ref[pl.ds(base + group_len // 2, slab), cols])
            depth = slab * (4 if t == 0 else 3)
            folded[pl.ds(base + pair * t, pair), cols] = jnp.dot(
                fold_ref[t, :, :depth], jnp.concatenate(taken, 0), preferred_element_type=F32
            ).astype(BF16)
        return carry

    lax.fori_loop(0, col_count * pieces, fold_step, 0)

    def arrived(ref, semaphore):
        pltpu.make_async_remote_copy(
            src_ref=ref, dst_ref=ref, send_sem=l_sem.at[0], recv_sem=semaphore,
            device_id=(other, c), device_id_type=MESH,
        ).wait_recv()

    def block_of(d, i):
        return 2 * lax.rem(z - d + chips, chips) + i

    stay1.wait()
    low_copy.wait()
    arrived(recv1.at[other], a_recv.at[0])
    for d in range(1, chips):
        for i in range(2):
            arrived(recv1.at[block_of(d, i)], a_recv.at[2 * d + i])
    tile = 32
    lane = lax.broadcasted_iota(jnp.int32, (tile, slab), 1)
    sine = (lane > half) | ((lane == half) & (r > 0))

    def turn_step(i, carry):
        rows = pl.ds(pl.multiple_of(i * tile, tile), tile)
        below = pl.ds(pl.multiple_of(block_len + i * tile, tile), tile)
        blocks = [recv1[a, rows, :].astype(F32) for a in range(row_count)]
        middle = row_count // 2
        even = [blocks[a] + blocks[row_count - a] for a in range(1, middle)]
        odd = [blocks[a] - blocks[row_count - a] for a in range(1, middle)]
        ends = (blocks[0] + blocks[middle], blocks[0] - blocks[middle])
        twist = twist_ref[rows, :]
        for q in range(middle + 1):
            real = ends[q % 2]
            imag = None
            for a in range(1, middle):
                angle = 2 * math.pi * (a * q % row_count) / row_count
                cosine, sinus = round(math.cos(angle), 12), round(math.sin(angle), 12)
                if cosine:
                    real = real + even[a - 1] * cosine
                if sinus:
                    term = odd[a - 1] * -sinus
                    imag = term if imag is None else imag + term
            for k, sign in ((q, 1.0), (row_count - q, -1.0)):
                if k == row_count or (sign < 0 and k == q):
                    continue
                cosine, sinus = twist[:, k : k + 1], twist[:, row_count + k : row_count + k + 1]
                if imag is None:
                    turned_real, turned_imag = real * cosine, -(real * sinus)
                else:
                    turned_real = real * cosine + imag * (sinus * sign)
                    turned_imag = imag * (cosine * sign) - real * sinus
                cols = pl.ds(k * slab, slab)
                stacked[rows, cols] = jnp.where(sine, -turned_imag, turned_real).astype(BF16)
                stacked[below, cols] = jnp.where(sine, turned_real, turned_imag).astype(BF16)
        return carry

    lax.fori_loop(0, block_len // tile, turn_step, 0)

    def lanes_of(index):
        return pl.ds(pl.multiple_of(index * slab, slab), slab)

    sends = []

    def share(origin, source, block, target, out_slot, in_slot):
        copy = pltpu.make_async_remote_copy(
            src_ref=source, dst_ref=lhs.at[origin, :, :, lanes_of(block)],
            send_sem=g_send.at[out_slot], recv_sem=g_recv.at[in_slot],
            device_id=(r, target), device_id_type=MESH,
        )
        copy.start()
        sends.append(copy)
        return copy

    def held(origin, block):
        return lhs.at[origin, :, :, lanes_of(block)]

    count = row_count
    from_x, from_y, from_far = [], [], []

    def offer(n, source, block):
        from_x.append(share(c, source, block, x_next, n, n))
        from_y.append(share(c, source, block, y_next, count + n, count + n))

    second_copies = []
    stay2 = pltpu.make_async_copy(send2.at[r], held(c, r), l_sem.at[1])
    near_first = sorted(range(chips), key=lambda d: min(d, chips - d))
    for d in near_first:
        chip = lax.rem(z + d, chips)
        lows = jnp.dot(
            low_ref[pl.ds(pl.multiple_of(chip * 2 * part, 2 * part), 2 * part), :], stacked[...],
            preferred_element_type=F32,
        ).astype(BF16)
        for i in range(2):
            for q in range(row_count):
                send2[2 * chip + i, q] = lows[i * part : (i + 1) * part, q * slab : (q + 1) * slab]
        for target, slot in ([(2 * chip, 2 * d), (2 * chip + 1, 2 * d + 1)] if d else [(other, 0)]):
            copy = pltpu.make_async_remote_copy(
                src_ref=send2.at[target], dst_ref=held(c, r),
                send_sem=b_send.at[slot],
                recv_sem=b_recv.at[slot] if d == 0 else b_recv.at[2 * d + r % 2],
                device_id=(target, c), device_id_type=MESH,
            )
            copy.start()
            second_copies.append(copy)
        if d == 0:
            offer(0, send2.at[r], r)
            stay2.start()

    pairs = [lax.rem(z - d + chips, chips) for d in near_first]
    order = [(None, r), (0, other)]
    for d in near_first[1:]:
        order += [(2 * d + i, block_of(d, i)) for i in range(2)]

    def multiply(origin, m, first=False, last=False):
        base = pl.multiple_of(origin * group_len + pairs[m] * pair, pair)
        taken = pl.ds(pl.multiple_of(pairs[m] * pair, pair), pair)

        def step(i, carry):
            cols = pl.ds(pl.multiple_of(i * wide, wide), wide)
            left = lhs[origin, :, :, taken].reshape(block_len, pair)
            value = jnp.dot(left, folded[pl.ds(base, pair), cols], preferred_element_type=F32)
            if not first:
                value = acc[:, cols] + value
            if not last:
                acc[:, cols] = value
            else:
                out_ref[:, :, cols] = value.astype(BF16).reshape(row_count, part, wide)
            return carry

        lax.fori_loop(0, pieces, step, 0)

    def own_part(m):
        if m == 0:
            stay2.wait()
        multiply(c, m, first=m == 0)

    def x_part(m):
        from_x[2 * m + 1].wait_recv()
        multiply(x_next, m)

    def y_part(m):
        from_y[2 * m].wait_recv()
        multiply(y_next, m)

    def far_part(m):
        from_far[2 * m].wait_recv()
        from_far[2 * m + 1].wait_recv()
        multiply(diagonal, m, last=m == chips - 1)

    for n in range(1, count + 1):
        if n < count:
            slot, block = order[n]
            arrived(held(c, block), b_recv.at[slot])
            offer(n, held(c, block), block)
        _, block = order[n - 1]
        slot = 2 * count + n - 1
        if n % 2:
            from_x[n - 1].wait_recv()
            from_far.append(share(x_next, held(x_next, block), block, y_next, slot, slot))
        else:
            from_y[n - 1].wait_recv()
            from_far.append(share(y_next, held(y_next, block), block, x_next, slot, slot))
        m = n // 2
        if n % 2:
            own_part(m)
            if m:
                x_part(m - 1)
        elif 2 <= m < chips:
            y_part(m - 2)
            if m >= 3:
                far_part(m - 3)
    y_part(chips - 2)
    for m in range(max(chips - 3, 0), chips - 2):
        far_part(m)
    x_part(chips - 1)
    y_part(chips - 1)
    far_part(chips - 2)
    far_part(chips - 1)

    for copy in sum_copies + first_copies + second_copies + sends:
        copy.wait_send()


def on_device_fused(tokens, norm_gain, out_weight):
    row_count = lax.axis_size("row")
    col_count = lax.axis_size("col")
    block_len, group_len = tokens.shape
    out_width = out_weight.shape[1]
    slab = group_len // row_count
    part = block_len // row_count
    chan_table, low_table, twist_cos, twist_sin = host_tables(group_len, row_count, block_len)
    twist = np.concatenate([twist_cos, twist_sin], 0).astype(np.float32)
    vmem = pl.BlockSpec(memory_space=pltpu.VMEM)
    dma = pltpu.SemaphoreType.DMA
    mapped = pl.pallas_call(
        functools.partial(fused_kernel, (row_count, col_count)),
        out_shape=jax.ShapeDtypeStruct((row_count, part, out_width), BF16),
        in_specs=[vmem] * 2 + [pl.BlockSpec(memory_space=pl.ANY)] * 4,
        out_specs=vmem,
        scratch_shapes=[
            pltpu.VMEM(chan_table.shape, BF16),
            pltpu.VMEM(low_table.shape, BF16),
            pltpu.VMEM(twist.shape, F32),
            pltpu.VMEM((block_len, 128), F32),
            pltpu.VMEM(out_weight.shape, BF16),
            pltpu.VMEM((row_count // 2, 2 * slab, 4 * slab), BF16),
            pltpu.VMEM(out_weight.shape, BF16),
            pltpu.VMEM((row_count, block_len, slab), BF16),
            pltpu.VMEM((row_count, block_len, slab), BF16),
            pltpu.VMEM((col_count, 8, block_len), F32),
            pltpu.VMEM((2 * block_len, row_count * slab), BF16),
            pltpu.VMEM((row_count, row_count, part, slab), BF16),
            pltpu.VMEM((col_count, row_count, part, group_len), BF16),
            pltpu.VMEM((block_len, out_width), F32),
            dma, dma((col_count - 1,)), dma((col_count - 1,)),
            dma((row_count,)), dma((row_count,)), dma((row_count,)), dma((row_count,)),
            dma((3 * row_count,)), dma((3 * row_count,)), dma((5,)),
        ],
        compiler_params=pltpu.CompilerParams(
            collective_id=0, has_side_effects=True, vmem_limit_bytes=60 * 1024 * 1024
        ),
    )(
        tokens, norm_gain[None, :], jnp.asarray(chan_table, BF16), jnp.asarray(low_table, BF16),
        jnp.asarray(twist), out_weight,
    )
    return jnp.transpose(mapped, (1, 0, 2)).reshape(block_len, out_width)


def on_device(tokens, norm_gain, out_weight):
    row_count = lax.axis_size("row")
    col_count = lax.axis_size("col")
    block_len, local_width = tokens.shape
    full_width = local_width * col_count
    group_len = full_width // GROUPS
    share_len = block_len // col_count
    seq_len = block_len * row_count
    slab_len = full_width // row_count
    col_index = lax.axis_index("col")
    chan_idx = jnp.arange(group_len, dtype=jnp.int32)
    cosines, sines = phases(chan_idx, chan_idx, group_len)
    chan_table = jnp.concatenate([cosines, sines], axis=1) / math.sqrt(group_len)
    table_parts = split_table(chan_table)
    arranged = tokens.reshape(col_count, share_len, local_width)
    portion = lax.all_to_all(arranged, "col", split_axis=0, concat_axis=2, tiled=True)
    item_count = portion.shape[1]
    values = portion.astype(jnp.float32)
    inv_rms = lax.rsqrt(jnp.mean(values * values, axis=-1, keepdims=True) + EPSILON)
    normed = lax.optimization_barrier((values * inv_rms * norm_gain).astype(jnp.bfloat16))
    grouped = normed.reshape(item_count, GROUPS, group_len)
    result = jnp.einsum("pgm,mj->pgj", grouped, table_parts[0], preferred_element_type=jnp.float32)
    result = result + jnp.einsum(
        "pgm,mj->pgj", grouped, table_parts[1], preferred_element_type=jnp.float32
    )
    result = result + jnp.einsum(
        "pgm,mj->pgj", grouped, table_parts[2], preferred_element_type=jnp.float32
    )
    high_idx = jnp.arange(row_count, dtype=jnp.int32)
    high_cos, high_sin = phases(high_idx, high_idx, row_count)
    high_table = jnp.concatenate(
        [jnp.concatenate([high_cos, -high_sin], 1), jnp.concatenate([-high_sin, -high_cos], 1)], 0
    )
    parts = (
        lax.all_to_all(
            result[..., :group_len].reshape(1, item_count, full_width),
            "row",
            split_axis=2,
            concat_axis=0,
            tiled=True,
        ),
        lax.all_to_all(
            result[..., group_len:].reshape(1, item_count, full_width),
            "row",
            split_axis=2,
            concat_axis=0,
            tiled=True,
        ),
    )
    item_count = parts[0].shape[1]
    stacked = jnp.concatenate(parts, 0).reshape(2 * row_count, item_count * slab_len)
    result = jnp.dot(high_table, stacked, precision=PRECISE)
    real_part = result[:row_count].reshape(row_count, item_count, slab_len)
    imag_part = result[row_count:].reshape(row_count, item_count, slab_len)
    local_pos = col_index * share_len + jnp.arange(share_len, dtype=jnp.int32)
    twist_cos, twist_sin = phases(high_idx, local_pos, seq_len)
    twist_cos = twist_cos[:, :, None]
    twist_sin = twist_sin[:, :, None]
    turned_real = real_part * twist_cos + imag_part * twist_sin
    turned_imag = imag_part * twist_cos - real_part * twist_sin
    low_idx = jnp.arange(block_len, dtype=jnp.int32)
    low_cos, low_sin = phases(low_idx, low_idx, block_len)
    low_cos = low_cos / math.sqrt(seq_len)
    low_sin = low_sin / math.sqrt(seq_len)
    low_table = jnp.concatenate([low_cos, low_sin], 1)
    stacked = jnp.concatenate(
        (
            lax.all_to_all(turned_real, "col", split_axis=0, concat_axis=1, tiled=True),
            lax.all_to_all(turned_imag, "col", split_axis=0, concat_axis=1, tiled=True),
        ),
        1,
    )
    finished = (jnp.einsum("ks,asc->akc", low_table, stacked, precision=PRECISE),)[0]
    spectrum = finished.astype(jnp.bfloat16)
    returned = lax.all_to_all(spectrum, "row", split_axis=1, concat_axis=2, tiled=True)
    mapped = jnp.einsum(
        "akd,de->kae",
        lax.all_gather(returned, "col", axis=0, tiled=True),
        out_weight,
        preferred_element_type=jnp.float32,
    )
    return mapped.astype(jnp.bfloat16).reshape(block_len, local_width)


def solution(mesh):
    def body(tokens, norm_gain, out_weight):
        whole_groups = tokens.shape[1] * GROUPS == out_weight.shape[0]
        slab = tokens.shape[1] // mesh.shape["row"]
        program = on_device_folded if whole_groups else on_device
        if whole_groups and slab == 128 and mesh.shape["col"] == 4 and mesh.shape["row"] == 8:
            program = on_device_fused
        return program(tokens, norm_gain, out_weight)

    placed = (P("row", "col"), P(), P(None, "col"))
    return jax.shard_map(
        body, mesh=mesh, in_specs=placed, out_specs=P("row", "col"), check_vma=False
    )
```
